128 devices in a mesh: sp: 64 (over z, y, x), tp: 2 (over core).
Axes of the slice: x: 4, y: 4, z: 4, core: 2. Of those that a mesh axis runs over, the one named last changes fastest.
Arguments:
- residual: bfloat16 [16384, 2048], P(('sp', 'tp')), may hold values from -6 to 6
- pool_input: bfloat16 [16384, 1024], P('sp', 'tp'), may hold values from -6 to 6
- group_maps: bfloat16 [8, 128, 128], replicated, may hold values from -0.5 to 0.5
- pool_scale: float32 [1024], replicated, may hold values from 0.1 to 1.9
- out_proj: bfloat16 [1024, 2048], replicated, may hold values from -0.1875 to 0.1875
- norm_gain: float32 [2048], replicated, may hold values from 0.1 to 1.9
- shared_gate: bfloat16 [2048, 512], replicated, may hold values from -0.125 to 0.125
- shared_up: bfloat16 [2048, 512], replicated, may hold values from -0.125 to 0.125
- shared_down: bfloat16 [512, 2048], replicated, may hold values from -0.25 to 0.25
- expert_gate: bfloat16 [128, 2048, 512], P(('sp', 'tp')), may hold values from -0.125 to 0.125
- expert_up: bfloat16 [128, 2048, 512], P(('sp', 'tp')), may hold values from -0.125 to 0.125
- expert_down: bfloat16 [128, 512, 2048], P(('sp', 'tp')), may hold values from -0.25 to 0.25
- expert_ids: int32 [16384, 4], P(('sp', 'tp')), may hold values from 0 to 127, all different within a row; in each aligned block of 128 rows (0 to 127, 128 to 255, ...) at most 6 rows name the same one
- route_score: float32 [16384, 4], P(('sp', 'tp')), may hold values from 0.05 to 1
Outputs:
- output: bfloat16 [16384, 2048], P(('sp', 'tp'))
The draws below stay inside these ranges and needn't reach their ends.
Inputs may be any that keep to these rules, and one draw needn't show every extreme that they name: `expert_ids`: each row names 4 different experts; among the 128 rows of one device no expert is named more than 6 times, and in some devices' rows one expert is named exactly 6 times.
All inputs are finite; a program needn't handle non-finite values.
Results may differ from the reference program's by a relative error of at most 0.015.
Values may be sent and summed in bfloat16 or wider, within the bound.
A program may use at most 128 MiB of HBM per device.

```python
import math
import jax
import jax.numpy as jnp
import numpy as np
from jax import lax

D = 2048
POOL_GROUPS = 8
GROUP_WIDTH = 128
EXPERT_HIDDEN = 512
SHARED_HIDDEN = 512
TOPK = 4
TOK_DEV = 128
TOKENS = 16384
POOL = 1024
EXPERTS = 128
CAP = 6


def shard_levels(own_key, shape, shards, least, high):
    def one(position, parts):
        draws = jax.random.uniform(jax.random.fold_in(jax.random.fold_in(own_key, 6), position), (parts,), jnp.float32, least / len(shards), high / len(shards))
        return jnp.repeat(jnp.exp(draws), shape[position] // parts).reshape((-1,) + (1,) * (len(shape) - position - 1))

    gain = one(*shards[0])
    for cut in shards[1:]:
        gain = gain * one(*cut)
    return gain


def shared_out(stream_key, own, number, rows, amount, top, reach, lean):
    ranking = jax.random.permutation(stream_key, amount)
    heavy_load, common = portions_of(amount, rows * top, reach, lean, True), portions_of(amount, rows * top, reach, lean, False)
    places = jnp.arange(amount)

    def named(tallies, rotation):
        used = int((tallies > 0).sum())
        fixed = max(1, used // 4)
        moved = fixed + (places - fixed + rotation * (used - fixed)) % max(1, amount - fixed)
        return jnp.zeros((amount,), jnp.int32).at[ranking[jnp.where(places < fixed, places, moved)]].set(jnp.asarray(tallies, jnp.int32))

    tallies = jnp.where(number % 4 == 0, named(heavy_load, number // 4), named(common, number - number // 4 - 1))
    mixed = jax.random.permutation(jax.random.fold_in(own, 3), amount)
    source_of, taker = mixed[0:amount // 2 * 2:2], mixed[1:amount // 2 * 2:2]
    slack = jnp.minimum(tallies[source_of] - 1, reach - tallies[taker]) // 2
    slack = jnp.where((source_of == ranking[0]) | (taker == ranking[0]) | (tallies[taker] == 0), 0, jnp.maximum(slack, 0))
    moved = jax.random.randint(jax.random.fold_in(own, 4), (amount // 2,), 0, 1 << 20) % (slack + 1)
    tallies = tallies.at[source_of].add(-moved).at[taker].add(moved)
    items = jnp.searchsorted(jnp.cumsum(tallies), jnp.arange(rows * top), side="right").astype(jnp.int32)
    table = items.reshape(top, rows).T
    table = table[jax.random.permutation(jax.random.fold_in(own, 1), rows)]
    rotation = jax.random.randint(jax.random.fold_in(own, 2), (rows, 1), 0, top)
    return jnp.take_along_axis(table, (jnp.arange(top)[None, :] + rotation) % top, axis=1)


def portions_of(count, total, bound, slope, full):
    loads = [(1 << 20) // math.isqrt(rank ** slope) + 1 for rank in range(1, count + 1)]
    largest = bound if full else min(bound, max(-(-total // count), total * loads[0] // sum(loads)))
    least = 1 if total - largest >= count - 1 else 0
    given, rest = [largest] + [least] * (count - 1), total - largest - least * (count - 1)
    while rest > 0:
        free = [i for i in range(1, count) if given[i] < largest] or [i for i in range(1, count) if given[i] < bound]
        mass, budget = sum([loads[i] for i in free]), rest
        for i in free:
            more = min(bound - given[i], max(1, budget * loads[i] // mass), rest)
            given[i] = given[i] + more
            rest = rest - more
    return np.array(given)


def bell_draw(stream_key, shape, spread, bound, shards=(), kind=jnp.bfloat16):
    drawn = spread * jax.random.normal(stream_key, shape, jnp.float32)
    if shards:
        drawn = drawn * shard_levels(stream_key, shape, shards, -0.22, 0.18)
    return jnp.clip(drawn, -bound, bound).astype(kind)


def setup_inputs(seed: int = 0) -> dict:
    keys = jax.random.split(jax.random.key(seed), 15)
    residual = bell_draw(keys[0], (TOKENS, D), 1.0, 6.0, ((0, 128),))
    pool_input = bell_draw(keys[1], (TOKENS, POOL), 1.0, 6.0, ((0, 64), (1, 2)))
    group_maps = bell_draw(keys[2], (POOL_GROUPS, GROUP_WIDTH, GROUP_WIDTH), GROUP_WIDTH ** -0.5, 0.5)
    pool_scale = jnp.clip(1.0 + 0.18 * jax.random.normal(keys[3], (POOL,), jnp.float32), 0.1, 1.9)
    out_proj = bell_draw(keys[4], (POOL, D), POOL ** -0.5, 0.1875)
    norm_gain = jnp.clip(1.0 + 0.18 * jax.random.normal(keys[5], (D,), jnp.float32), 0.1, 1.9)
    shared_gate = bell_draw(keys[6], (D, SHARED_HIDDEN), D ** -0.5, 0.125)
    shared_up = bell_draw(keys[7], (D, SHARED_HIDDEN), D ** -0.5, 0.125)
    shared_down = bell_draw(keys[8], (SHARED_HIDDEN, D), SHARED_HIDDEN ** -0.5, 0.25)
    expert_gate = bell_draw(keys[9], (EXPERTS, D, EXPERT_HIDDEN), D ** -0.5, 0.125, ((0, 128),))
    expert_up = bell_draw(keys[10], (EXPERTS, D, EXPERT_HIDDEN), D ** -0.5, 0.125, ((0, 128),))
    expert_down = bell_draw(keys[11], (EXPERTS, EXPERT_HIDDEN, D), EXPERT_HIDDEN ** -0.5, 0.25, ((0, 128),))
    expert_ids_keys = jax.random.split(jax.random.fold_in(keys[12], 1), TOKENS // TOK_DEV)
    expert_ids_turns = jax.random.permutation(jax.random.fold_in(keys[12], 3), TOKENS // TOK_DEV)
    expert_ids = jax.vmap(lambda own, number: shared_out(jax.random.fold_in(keys[12], 2), own, number, TOK_DEV, EXPERTS, TOPK, CAP, 2))(expert_ids_keys, expert_ids_turns).reshape((TOKENS, TOPK))
    route_score = jnp.clip(0.05 + 0.95 * jax.random.uniform(keys[13], (TOKENS, TOPK), jnp.float32) ** shard_levels(keys[13], (TOKENS, TOPK), ((0, 128),), -0.2, 0.2), 0.05, 1.0)
    return dict(residual=residual, pool_input=pool_input, group_maps=group_maps, pool_scale=pool_scale, out_proj=out_proj, norm_gain=norm_gain, shared_gate=shared_gate, shared_up=shared_up, shared_down=shared_down, expert_gate=expert_gate, expert_up=expert_up, expert_down=expert_down, expert_ids=expert_ids, route_score=route_score)


windows = (2, 4, 8, 16)
epsilon = 1e-06
routed_scale = 2.5

def swiglu(row_block, w_gate, w_up, w_down):
    gate_part = jnp.dot(row_block, w_gate, preferred_element_type=jnp.float32)
    up_part = jnp.dot(row_block, w_up, preferred_element_type=jnp.float32)
    hidden = (jax.nn.silu(gate_part) * up_part).astype(jnp.bfloat16)
    return jnp.dot(hidden, w_down, preferred_element_type=jnp.float32)

def reference(residual, pool_input, group_maps, pool_scale, out_proj, norm_gain, shared_gate, shared_up, shared_down, expert_gate, expert_up, expert_down, expert_ids, route_score):
    length = pool_input.shape[0]
    groups = group_maps.shape[0]
    group_width = group_maps.shape[1]
    input_values = pool_input.astype(jnp.float32).reshape(length, groups, group_width)
    places = jnp.arange(length, dtype=jnp.int32)
    pooled = []
    for group_index in range(groups):
        window_span = windows[group_index % 4]
        group_column = input_values[:, group_index]
        padded = jnp.pad(group_column, ((window_span - 1, 0), (0, 0)))
        running_sum = padded[window_span - 1:]
        for offset_shift in range(1, window_span):
            running_sum = running_sum + padded[window_span - 1 - offset_shift:window_span - 1 - offset_shift + length]
        divisor = jnp.minimum(places + 1, window_span).astype(jnp.float32)[:, None]
        pooled.append(running_sum / divisor)
    pooled = jnp.stack(pooled, axis=1)
    contrast = (pooled - input_values).astype(jnp.bfloat16)
    mapped = jnp.einsum('sgc,gcd->sgd', contrast.astype(jnp.float32), group_maps.astype(jnp.float32))
    mixed_rows = (mapped.reshape(length, groups * group_width) * pool_scale).astype(jnp.bfloat16)
    projected = jnp.dot(mixed_rows, out_proj, preferred_element_type=jnp.float32)
    settled = (residual.astype(jnp.float32) + projected).astype(jnp.bfloat16)
    settled_wide = settled.astype(jnp.float32)
    inverse_rms = lax.rsqrt(lax.optimization_barrier(jnp.mean(settled_wide * settled_wide, axis=-1, keepdims=True)) + epsilon)
    normed = (settled_wide * inverse_rms * norm_gain).astype(jnp.bfloat16)
    shared = swiglu(normed, shared_gate, shared_up, shared_down)
    weights = route_score / lax.optimization_barrier(jnp.sum(route_score, axis=-1, keepdims=True)) * routed_scale
    experts = expert_gate.shape[0]
    top_count = expert_ids.shape[1]
    assigned = length * top_count
    flat_ids = expert_ids.reshape(assigned).astype(jnp.int32)
    sort_order = jnp.argsort(flat_ids, stable=True).astype(jnp.int32)
    sorted_ids = flat_ids[sort_order]
    counts = jnp.bincount(flat_ids, length=experts).astype(jnp.int32)
    starts = jnp.cumsum(counts).astype(jnp.int32) - counts
    expert_depth = EXPERTS * CAP
    slot_rank = jnp.arange(assigned, dtype=jnp.int32) - starts[sorted_ids]
    slot_index = sorted_ids * expert_depth + slot_rank
    slot_token = jnp.zeros((experts * expert_depth,), jnp.int32).at[slot_index].set(sort_order // top_count)
    slot_weight = jnp.zeros((experts * expert_depth,), jnp.float32).at[slot_index].set(weights.reshape(assigned)[sort_order])

    def one_expert(routed, inputs):
        token_index, slot_factor, w_gate, w_up, w_down = inputs
        expert_rows = swiglu(normed[token_index], w_gate, w_up, w_down).astype(jnp.bfloat16)
        return (routed.at[token_index].add(slot_factor[:, None] * expert_rows.astype(jnp.float32)), None)
    routed, _ = lax.scan(one_expert, jnp.zeros((length, D), jnp.float32), (slot_token.reshape(experts, expert_depth), slot_weight.reshape(experts, expert_depth), expert_gate, expert_up, expert_down))
    return (settled_wide + shared + routed).astype(jnp.bfloat16)
```

```python
import functools

import jax
import jax.numpy as jnp
from jax import lax
from jax.experimental import pallas as pl
from jax.experimental.pallas import tpu as pltpu
from jax.sharding import PartitionSpec as P

windows = (2, 4, 8, 16)
epsilon = 1e-06
routed_scale = 2.5

MESH = pl.DeviceIdType.MESH
F32 = jnp.float32
BF16 = jnp.bfloat16

SIDE = 4
DEVICES = 128
TOKENS_HERE = 128
TOPK = 4
CAP = 6
SLOTS = 8
D = 2048
HID = 512
ROWS = 256
CHANNELS = 512
GROUPS = 4
GW = 128
REACH = 16
STRIDE = 53
PARTS = 4
PEERS = DEVICES // PARTS


def dot(a, b):
    return jnp.dot(a, b, preferred_element_type=F32)


def offset_of(k):
    kk = lax.rem(k * STRIDE, DEVICES)
    c = lax.rem(kk, 2)
    x = lax.rem(lax.div(kk, 2), SIDE)
    y = lax.rem(lax.div(kk, 8), SIDE)
    z = lax.div(kk, 32)
    return z, y, x, c


def shifted(sp, tp, k, sign):
    dz, dy, dx, dc = offset_of(k)
    z = lax.div(sp, SIDE * SIDE)
    y = lax.rem(lax.div(sp, SIDE), SIDE)
    x = lax.rem(sp, SIDE)
    z = lax.rem(z + sign * dz + SIDE, SIDE)
    y = lax.rem(y + sign * dy + SIDE, SIDE)
    x = lax.rem(x + sign * dx + SIDE, SIDE)
    c = lax.rem(tp + dc, 2)
    return (z * SIDE + y) * SIDE + x, c


def kernel(
    res_hbm, pool_hbm, maps_hbm, scale_hbm, proj_hbm, gain_hbm,
    sg_hbm, su_hbm, sd_hbm, eg_hbm, eu_hbm, ed_hbm, ids_hbm, score_hbm,
    out_ref,
    res, ext, maps, scale, proj, gain, sg, su, sd, eg, eu, ed, ids, score,
    mix, halves, settled, normed, acc, place, comb,
    outgoing, arrived, results, returned,
    in_sems, halo_send, halo_recv, swap_send, swap_recv,
    out_send, out_recv, back_send, back_recv,
):
    sp = lax.axis_index("sp")
    tp = lax.axis_index("tp")

    def fetch(i, src, dst):
        copy = pltpu.make_async_copy(src, dst, in_sems.at[i])
        copy.start()
        return copy

    get_pool = fetch(0, pool_hbm, ext.at[pl.ds(REACH, ROWS)])
    get_ids = fetch(1, ids_hbm, ids)
    get_score = fetch(2, score_hbm, score)
    get_maps = fetch(3, maps_hbm.at[pl.ds(tp * GROUPS, GROUPS)], maps)
    get_scale = fetch(4, scale_hbm, scale)
    get_res = fetch(5, res_hbm, res)
    get_gain = fetch(6, gain_hbm, gain)
    get_proj = fetch(7, proj_hbm, proj)
    get_sg = fetch(8, sg_hbm, sg)
    get_su = fetch(9, su_hbm, su)
    get_sd = fetch(10, sd_hbm, sd)
    get_eg = fetch(11, eg_hbm.at[0], eg)
    get_eu = fetch(12, eu_hbm.at[0], eu)
    get_ed = fetch(13, ed_hbm.at[0], ed)

    def clear(i, _):
        returned[pl.ds(i * 8, 8)] = jnp.zeros((8, SLOTS, D), BF16)
        return 0

    lax.fori_loop(0, DEVICES // 8, clear, 0)

    barrier = pltpu.get_barrier_semaphore()

    def greet(k, _):
        pl.semaphore_signal(barrier, inc=1, device_id=shifted(sp, tp, k, 1), device_id_type=MESH)
        return 0

    lax.fori_loop(1, DEVICES, greet, 0)
    get_pool.wait()
    pl.semaphore_wait(barrier, DEVICES - 1)

    halo = pltpu.make_async_remote_copy(
        ext.at[pl.ds(ROWS, REACH)], ext.at[pl.ds(0, REACH)], halo_send, halo_recv,
        device_id=(lax.rem(sp + 1, DEVICES // 2), tp), device_id_type=MESH,
    )
    halo.start()

    get_ids.wait()
    get_score.wait()
    expert = lax.broadcasted_iota(jnp.int32, (DEVICES, TOKENS_HERE), 0)
    raw = score[...]
    weights = raw / jnp.sum(raw, axis=0, keepdims=True) * routed_scale
    chosen = jnp.zeros((DEVICES, TOKENS_HERE), F32)
    weight = jnp.zeros((DEVICES, TOKENS_HERE), F32)
    for k in range(TOPK):
        hit = expert == ids[k : k + 1, :]
        chosen = jnp.where(hit, 1.0, chosen)
        weight = jnp.where(hit, weights[k : k + 1, :], weight)
    row = lax.broadcasted_iota(jnp.int32, (TOKENS_HERE, TOKENS_HERE), 0)
    column = lax.broadcasted_iota(jnp.int32, (TOKENS_HERE, TOKENS_HERE), 1)
    earlier = (row < column).astype(BF16)
    rank = dot(chosen.astype(BF16), earlier)
    tag = chosen * (rank + 1.0)
    slot_row = lax.broadcasted_iota(jnp.int32, (DEVICES * SLOTS, DEVICES), 0)
    slot_expert = lax.broadcasted_iota(jnp.int32, (DEVICES * SLOTS, DEVICES), 1)
    peer_sp, peer_tp = shifted(sp, tp, lax.div(slot_row, SLOTS), 1)
    spread = (peer_sp * 2 + peer_tp == slot_expert).astype(BF16)
    slot_number = (lax.rem(slot_row, SLOTS) + 1).astype(F32)
    place[...] = (dot(spread, tag.astype(BF16)) == slot_number).astype(BF16)
    weight_high = weight.astype(BF16)
    weight_low = (weight - weight_high.astype(F32)).astype(BF16)
    comb[:, :TOKENS_HERE] = dot(spread, weight_high).astype(BF16) * place[...]
    comb[:, TOKENS_HERE:] = dot(spread, weight_low).astype(BF16) * place[...]

    get_maps.wait()
    get_scale.wait()
    halo.wait()
    center = lax.broadcasted_iota(jnp.int32, (ROWS, REACH + ROWS), 0) + REACH
    other = lax.broadcasted_iota(jnp.int32, (ROWS, REACH + ROWS), 1)
    real = (other >= REACH) | (sp > 0)
    position = sp * ROWS + lax.broadcasted_iota(jnp.int32, (ROWS, GW), 0)
    for g in range(GROUPS):
        lanes = slice(g * GW, (g + 1) * GW)
        band = (other <= center) & (other > center - windows[g]) & real
        total = dot(band.astype(BF16), ext[:, lanes])
        divisor = jnp.minimum(position + 1, windows[g]).astype(F32)
        contrast = (total / divisor - ext[REACH:, lanes].astype(F32)).astype(BF16)
        mapped = dot(contrast, maps[g])
        row_scale = jnp.where(tp == 0, scale[g : g + 1, :], scale[GROUPS + g : GROUPS + g + 1, :])
        mix[:, lanes] = (mapped * row_scale).astype(BF16)

    swap = pltpu.make_async_remote_copy(
        mix.at[pl.ds(pl.multiple_of((1 - tp) * TOKENS_HERE, TOKENS_HERE), TOKENS_HERE)],
        halves, swap_send, swap_recv, device_id=(sp, 1 - tp), device_id_type=MESH,
    )
    swap.start()

    get_res.wait()
    get_gain.wait()
    get_proj.wait()
    own = mix[pl.ds(pl.multiple_of(tp * TOKENS_HERE, TOKENS_HERE), TOKENS_HERE), :]
    for n in range(0, D, 512):
        near = proj[pl.ds(pl.multiple_of(tp * CHANNELS, CHANNELS), CHANNELS), n : n + 512]
        acc[:, n : n + 512] = dot(own, near)
    swap.wait()
    square = jnp.zeros((TOKENS_HERE, 1), F32)
    for n in range(0, D, 512):
        far = proj[pl.ds(pl.multiple_of((1 - tp) * CHANNELS, CHANNELS), CHANNELS), n : n + 512]
        value = acc[:, n : n + 512] + dot(halves[...], far)
        value = (value + res[:, n : n + 512].astype(F32)).astype(BF16)
        settled[:, n : n + 512] = value
        value = value.astype(F32)
        square = square + jnp.sum(value * value, axis=1, keepdims=True)
    inverse = lax.rsqrt(square / D + epsilon)
    for j in range(D // 128):
        lanes = slice(j * 128, (j + 1) * 128)
        value = settled[:, lanes].astype(F32) * inverse * gain[j : j + 1, :]
        normed[:, lanes] = value.astype(BF16)

    def fill(i, _):
        n = pl.multiple_of(i * 256, 256)
        rows = dot(place[...], normed[:, pl.ds(n, 256)]).astype(BF16)
        outgoing[:, :, pl.ds(n, 256)] = rows.reshape(DEVICES, SLOTS, 256)
        return 0

    lax.fori_loop(0, D // 256, fill, 0)

    def send(k, part):
        pltpu.make_async_remote_copy(
            outgoing.at[k, pl.ds(0, CAP)], arrived.at[k, pl.ds(0, CAP)],
            out_send, out_recv.at[part],
            device_id=shifted(sp, tp, k, 1), device_id_type=MESH,
        ).start()
        return part

    def send_back(k, part):
        pltpu.make_async_remote_copy(
            results.at[k, pl.ds(0, CAP)], returned.at[k, pl.ds(0, CAP)],
            back_send, back_recv.at[part],
            device_id=shifted(sp, tp, k, -1), device_id_type=MESH,
        ).start()
        return part

    for part in range(PARTS):
        lax.fori_loop(max(part * PEERS, 1), (part + 1) * PEERS, send, part)
    arrived[0] = outgoing[0]

    get_sg.wait()
    get_su.wait()
    get_sd.wait()
    hidden = dot(normed[...], sg[...])
    hidden = hidden / (1.0 + jnp.exp(-hidden)) * dot(normed[...], su[...])
    hidden = hidden.astype(BF16)
    for n in range(0, D, 512):
        acc[:, n : n + 512] = settled[:, n : n + 512].astype(F32) + dot(hidden, sd[:, n : n + 512])

    get_eg.wait()
    get_eu.wait()
    get_ed.wait()

    def span(refs, sems_send, sem_recv, first, count):
        src, dst = refs
        return pltpu.make_async_remote_copy(
            src.at[pl.ds(first, count), pl.ds(0, CAP)], dst.at[pl.ds(first, count), pl.ds(0, CAP)],
            sems_send, sem_recv, device_id=(sp, 1 - tp), device_id_type=MESH,
        )

    for part in range(PARTS):
        first = max(part * PEERS, 1)
        count = (part + 1) * PEERS - first
        span((outgoing, arrived), out_send, out_recv.at[part], first, count).wait_recv()
        base = part * PEERS
        rows = arrived[pl.ds(base, PEERS)].reshape(PEERS * SLOTS, D)
        hidden = dot(rows, eg[...])
        hidden = hidden / (1.0 + jnp.exp(-hidden)) * dot(rows, eu[...])
        hidden = hidden.astype(BF16)
        for n in range(0, D, 512):
            value = dot(hidden, ed[:, n : n + 512]).astype(BF16)
            results[pl.ds(base, PEERS), :, n : n + 512] = value.reshape(PEERS, SLOTS, 512)
        lax.fori_loop(first, base + PEERS, send_back, part)
    returned[0] = results[0]

    for part in range(PARTS):
        first = max(part * PEERS, 1)
        count = (part + 1) * PEERS - first
        span((results, returned), back_send, back_recv.at[part], first, count).wait_recv()
        base = part * PEERS
        factors = comb[pl.ds(base * SLOTS, PEERS * SLOTS), :].T
        for n in range(0, D, 512):
            rows = returned[pl.ds(base, PEERS), :, n : n + 512].reshape(PEERS * SLOTS, 512)
            both = dot(factors, rows)
            value = acc[:, n : n + 512] + (both[:TOKENS_HERE] + both[TOKENS_HERE:])
            if part < PARTS - 1:
                acc[:, n : n + 512] = value
            else:
                out_ref[:, n : n + 512] = value.astype(BF16)

    span((outgoing, arrived), out_send, out_recv.at[0], 1, DEVICES - 1).wait_send()
    span((results, returned), back_send, back_recv.at[0], 1, DEVICES - 1).wait_send()


def on_device(
    residual, pool_input, group_maps, pool_scale, out_proj, norm_gain,
    shared_gate, shared_up, shared_down, expert_gate, expert_up, expert_down,
    expert_ids, route_score,
):
    any_space = pl.BlockSpec(memory_space=pl.ANY)
    vmem = pltpu.VMEM
    block = (DEVICES, SLOTS, D)
    return pl.pallas_call(
        kernel,
        name="mixer_experts",
        out_shape=jax.ShapeDtypeStruct((TOKENS_HERE, D), BF16),
        in_specs=[any_space] * 14,
        out_specs=pl.BlockSpec(memory_space=pltpu.VMEM),
        scratch_shapes=[
            vmem((TOKENS_HERE, D), BF16),
            vmem((REACH + ROWS, CHANNELS), BF16),
            vmem((GROUPS, GW, GW), BF16),
            vmem((8, 128), F32),
            vmem((2 * CHANNELS, D), BF16),
            vmem((D // 128, 128), F32),
            vmem((D, HID), BF16),
            vmem((D, HID), BF16),
            vmem((HID, D), BF16),
            vmem((D, HID), BF16),
            vmem((D, HID), BF16),
            vmem((HID, D), BF16),
            vmem((TOPK, TOKENS_HERE), jnp.int32),
            vmem((TOPK, TOKENS_HERE), F32),
            vmem((ROWS, CHANNELS), BF16),
            vmem((TOKENS_HERE, CHANNELS), BF16),
            vmem((TOKENS_HERE, D), BF16),
            vmem((TOKENS_HERE, D), BF16),
            vmem((TOKENS_HERE, D), F32),
            vmem((DEVICES * SLOTS, TOKENS_HERE), BF16),
            vmem((DEVICES * SLOTS, 2 * TOKENS_HERE), BF16),
            vmem(block, BF16),
            vmem(block, BF16),
            vmem(block, BF16),
            vmem(block, BF16),
            pltpu.SemaphoreType.DMA((14,)),
            pltpu.SemaphoreType.DMA,
            pltpu.SemaphoreType.DMA,
            pltpu.SemaphoreType.DMA,
            pltpu.SemaphoreType.DMA,
            pltpu.SemaphoreType.DMA,
            pltpu.SemaphoreType.DMA((PARTS,)),
            pltpu.SemaphoreType.DMA,
            pltpu.SemaphoreType.DMA((PARTS,)),
        ],
        compiler_params=pltpu.CompilerParams(
            collective_id=0, has_side_effects=True, vmem_limit_bytes=60 << 20
        ),
    )(
        residual, pool_input, group_maps, pool_scale.reshape(8, 128), out_proj,
        norm_gain.reshape(D // 128, 128), shared_gate, shared_up, shared_down,
        expert_gate, expert_up, expert_down, expert_ids.T, route_score.T,
    )


def solution(mesh):
    in_specs = (
        P(("sp", "tp"), None),
        P("sp", "tp"),
        P(), P(), P(), P(), P(), P(), P(),
        P(("sp", "tp"), None, None),
        P(("sp", "tp"), None, None),
        P(("sp", "tp"), None, None),
        P(("sp", "tp"), None),
        P(("sp", "tp"), None),
    )
    return jax.shard_map(
        on_device, mesh=mesh, in_specs=in_specs, out_specs=P(("sp", "tp"), None), check_vma=False
    )
```

```python
import functools

import jax
import jax.numpy as jnp
from jax import lax
from jax.experimental import pallas as pl
from jax.experimental.pallas import tpu as pltpu
from jax.sharding import PartitionSpec as P

windows = (2, 4, 8, 16)
epsilon = 1e-06
routed_scale = 2.5

MESH = pl.DeviceIdType.MESH
F32 = jnp.float32
BF16 = jnp.bfloat16

SIDE = 4
DEVICES = 128
TOKENS_HERE = 128
TOPK = 4
CAP = 6
SLOTS = 8
D = 2048
HID = 512
ROWS = 256
CHANNELS = 512
GROUPS = 4
GW = 128
REACH = 16
STRIDE = 53
PARTS = (32, 32, 32, 16, 16)


def members(part):
    first = sum(PARTS[:part])
    return range(max(first, 1), first + PARTS[part])


def dot(a, b):
    return jnp.dot(a, b, preferred_element_type=F32)


def offset_of(k):
    kk = k * STRIDE % DEVICES
    return kk // 32, kk // 8 % SIDE, kk // 2 % SIDE, kk % 2


class Place:
    def __init__(self):
        self.sp = lax.axis_index("sp")
        self.tp = lax.axis_index("tp")
        z, y, x = self.sp // 16, self.sp // SIDE % SIDE, self.sp % SIDE
        self.z = [(z + d) % SIDE * 16 for d in range(SIDE)]
        self.y = [(y + d) % SIDE * SIDE for d in range(SIDE)]
        self.x = [(x + d) % SIDE for d in range(SIDE)]
        self.c = [self.tp, 1 - self.tp]

    def at(self, dz, dy, dx, dc):
        return self.z[dz % SIDE] + self.y[dy % SIDE] + self.x[dx % SIDE], self.c[dc]

    def peer(self, k, sign):
        dz, dy, dx, dc = offset_of(k)
        return self.at(sign * dz, sign * dy, sign * dx, dc)


def kernel(
    res_hbm, pool_hbm, maps_hbm, scale_hbm, proj_hbm, gain_hbm,
    sg_hbm, su_hbm, sd_hbm, eg_hbm, eu_hbm, ed_hbm, ids_hbm, score_hbm,
    out_ref,
    res, ext, maps, scale, proj, gain, sg, su, sd, eg, eu, ed, ids, score,
    mix, halves, settled, normed, acc, place, comb,
    outgoing, arrived, results, returned,
    in_sems, halo_send, halo_recv, swap_send, swap_recv,
    out_send, out_recv, back_send, back_recv, plane_sem, cube_sem,
):
    here = Place()
    sp, tp = here.sp, here.tp

    def fetch(i, src, dst):
        copy = pltpu.make_async_copy(src, dst, in_sems.at[i])
        copy.start()
        return copy

    get_pool = fetch(0, pool_hbm, ext.at[pl.ds(REACH, ROWS)])
    get_ids = fetch(1, ids_hbm, ids)
    get_score = fetch(2, score_hbm, score)
    get_maps = fetch(3, maps_hbm.at[pl.ds(tp * GROUPS, GROUPS)], maps)
    get_scale = fetch(4, scale_hbm, scale)
    get_res = fetch(5, res_hbm, res)
    get_gain = fetch(6, gain_hbm, gain)
    get_proj = fetch(7, proj_hbm, proj)
    get_sg = fetch(8, sg_hbm, sg)
    get_su = fetch(9, su_hbm, su)
    get_sd = fetch(10, sd_hbm, sd)
    get_eg = fetch(11, eg_hbm.at[0], eg)
    get_eu = fetch(12, eu_hbm.at[0], eu)
    get_ed = fetch(13, ed_hbm.at[0], ed)

    barrier = pltpu.get_barrier_semaphore()
    near = [here.at(0, 0, d // 2, d % 2) for d in range(1, 2 * SIDE)]
    near += [here.at(0, d, 0, 0) for d in range(1, SIDE)]
    near += [here.at(d, 0, 0, 0) for d in range(1, SIDE)]
    following = (sp + 1) % (DEVICES // 2)
    near += [(following, tp), ((sp + DEVICES // 2 - 1) % (DEVICES // 2), tp)]
    for device in near:
        pl.semaphore_signal(barrier, inc=1, device_id=device, device_id_type=MESH)

    def clear(i, _):
        returned[pl.ds(i * 8, 8), CAP:, :] = jnp.zeros((8, SLOTS - CAP, D), BF16)
        return 0

    lax.fori_loop(0, DEVICES // 8, clear, 0)
    get_pool.wait()
    pl.semaphore_wait(barrier, len(near))

    halo = pltpu.make_async_remote_copy(
        ext.at[pl.ds(ROWS, REACH)], ext.at[pl.ds(0, REACH)], halo_send, halo_recv,
        device_id=(following, tp), device_id_type=MESH,
    )
    halo.start()
    for d in range(1, SIDE):
        pl.semaphore_signal(plane_sem, inc=1, device_id=here.at(0, d, 0, 0), device_id_type=MESH)

    get_ids.wait()
    get_score.wait()
    expert = lax.broadcasted_iota(jnp.int32, (DEVICES, TOKENS_HERE), 0)
    raw = score[...]
    weights = raw / jnp.sum(raw, axis=0, keepdims=True) * routed_scale
    chosen = jnp.zeros((DEVICES, TOKENS_HERE), F32)
    weight = jnp.zeros((DEVICES, TOKENS_HERE), F32)
    for k in range(TOPK):
        hit = expert == ids[k : k + 1, :]
        chosen = jnp.where(hit, 1.0, chosen)
        weight = jnp.where(hit, weights[k : k + 1, :], weight)
    row = lax.broadcasted_iota(jnp.int32, (TOKENS_HERE, TOKENS_HERE), 0)
    column = lax.broadcasted_iota(jnp.int32, (TOKENS_HERE, TOKENS_HERE), 1)
    earlier = (row < column).astype(BF16)
    rank = dot(chosen.astype(BF16), earlier)
    tag = chosen * (rank + 1.0)
    slot_row = lax.broadcasted_iota(jnp.int32, (DEVICES * SLOTS, DEVICES), 0)
    slot_expert = lax.broadcasted_iota(jnp.int32, (DEVICES * SLOTS, DEVICES), 1)
    turn = (slot_row // SLOTS) * STRIDE % DEVICES
    peer_z = (sp // 16 + turn // 32) % SIDE
    peer_y = (sp // SIDE + turn // 8) % SIDE
    peer_x = (sp + turn // 2) % SIDE
    peer = ((peer_z * SIDE + peer_y) * SIDE + peer_x) * 2 + (tp + turn) % 2
    spread = (peer == slot_expert).astype(BF16)
    slot_number = (slot_row % SLOTS + 1).astype(F32)
    place[...] = (dot(spread, tag.astype(BF16)) == slot_number).astype(BF16)
    weight_high = weight.astype(BF16)
    weight_low = (weight - weight_high.astype(F32)).astype(BF16)
    comb[:, :TOKENS_HERE] = dot(spread, weight_high).astype(BF16) * place[...]
    comb[:, TOKENS_HERE:] = dot(spread, weight_low).astype(BF16) * place[...]

    pl.semaphore_wait(plane_sem, SIDE - 1)
    for d in range(1, SIDE):
        pl.semaphore_signal(cube_sem, inc=1, device_id=here.at(d, 0, 0, 0), device_id_type=MESH)

    get_maps.wait()
    get_scale.wait()
    halo.wait()
    center = lax.broadcasted_iota(jnp.int32, (ROWS, REACH + ROWS), 0) + REACH
    other = lax.broadcasted_iota(jnp.int32, (ROWS, REACH + ROWS), 1)
    real = (other >= REACH) | (sp > 0)
    position = sp * ROWS + lax.broadcasted_iota(jnp.int32, (ROWS, GW), 0)
    for g in range(GROUPS):
        lanes = slice(g * GW, (g + 1) * GW)
        band = (other <= center) & (other > center - windows[g]) & real
        total = dot(band.astype(BF16), ext[:, lanes])
        divisor = jnp.minimum(position + 1, windows[g]).astype(F32)
        contrast = (total / divisor - ext[REACH:, lanes].astype(F32)).astype(BF16)
        mapped = dot(contrast, maps[g])
        row_scale = jnp.where(tp == 0, scale[g : g + 1, :], scale[GROUPS + g : GROUPS + g + 1, :])
        mix[:, lanes] = (mapped * row_scale).astype(BF16)

    swap = pltpu.make_async_remote_copy(
        mix.at[pl.ds(pl.multiple_of((1 - tp) * TOKENS_HERE, TOKENS_HERE), TOKENS_HERE)],
        halves, swap_send, swap_recv, device_id=(sp, 1 - tp), device_id_type=MESH,
    )
    swap.start()

    get_res.wait()
    get_gain.wait()
    get_proj.wait()
    own = mix[pl.ds(pl.multiple_of(tp * TOKENS_HERE, TOKENS_HERE), TOKENS_HERE), :]
    for n in range(0, D, 512):
        near = proj[pl.ds(pl.multiple_of(tp * CHANNELS, CHANNELS), CHANNELS), n : n + 512]
        acc[:, n : n + 512] = dot(own, near)
    swap.wait()
    square = jnp.zeros((TOKENS_HERE, 1), F32)
    for n in range(0, D, 512):
        far = proj[pl.ds(pl.multiple_of((1 - tp) * CHANNELS, CHANNELS), CHANNELS), n : n + 512]
        value = acc[:, n : n + 512] + dot(halves[...], far)
        value = (value + res[:, n : n + 512].astype(F32)).astype(BF16)
        settled[:, n : n + 512] = value
        value = value.astype(F32)
        square = square + jnp.sum(value * value, axis=1, keepdims=True)
    inverse = lax.rsqrt(square / D + epsilon)
    for j in range(D // 128):
        lanes = slice(j * 128, (j + 1) * 128)
        value = settled[:, lanes].astype(F32) * inverse * gain[j : j + 1, :]
        normed[:, lanes] = value.astype(BF16)

    def fill(i, _):
        n = pl.multiple_of(i * 256, 256)
        rows = dot(place[...], normed[:, pl.ds(n, 256)]).astype(BF16)
        outgoing[:, :, pl.ds(n, 256)] = rows.reshape(DEVICES, SLOTS, 256)
        return 0

    lax.fori_loop(0, D // 256, fill, 0)

    pl.semaphore_wait(cube_sem, SIDE - 1)
    for part in range(len(PARTS)):
        for k in members(part):
            pltpu.make_async_remote_copy(
                outgoing.at[k, pl.ds(0, CAP)], arrived.at[k, pl.ds(0, CAP)],
                out_send, out_recv.at[part],
                device_id=here.peer(k, 1), device_id_type=MESH,
            ).start()
    arrived[0] = outgoing[0]

    get_sg.wait()
    get_su.wait()
    get_sd.wait()
    hidden = dot(normed[...], sg[...])
    hidden = hidden / (1.0 + jnp.exp(-hidden)) * dot(normed[...], su[...])
    hidden = hidden.astype(BF16)
    for n in range(0, D, 512):
        acc[:, n : n + 512] = settled[:, n : n + 512].astype(F32) + dot(hidden, sd[:, n : n + 512])

    get_eg.wait()
    get_eu.wait()
    get_ed.wait()

    def span(src, dst, send_sem, recv_sem, first, count):
        return pltpu.make_async_remote_copy(
            src.at[pl.ds(first, count), pl.ds(0, CAP)], dst.at[pl.ds(first, count), pl.ds(0, CAP)],
            send_sem, recv_sem, device_id=(sp, 1 - tp), device_id_type=MESH,
        )

    base = 0
    for part, size in enumerate(PARTS):
        ks = members(part)
        span(outgoing, arrived, out_send, out_recv.at[part], ks[0], len(ks)).wait_recv()
        rows = arrived[pl.ds(base, size)].reshape(size * SLOTS, D)
        hidden = dot(rows, eg[...])
        hidden = hidden / (1.0 + jnp.exp(-hidden)) * dot(rows, eu[...])
        hidden = hidden.astype(BF16)
        for n in range(0, D, 512):
            value = dot(hidden, ed[:, n : n + 512]).astype(BF16)
            results[pl.ds(base, size), :, n : n + 512] = value.reshape(size, SLOTS, 512)
        for k in ks:
            pltpu.make_async_remote_copy(
                results.at[k, pl.ds(0, CAP)], returned.at[k, pl.ds(0, CAP)],
                back_send, back_recv.at[part],
                device_id=here.peer(k, -1), device_id_type=MESH,
            ).start()
        base += size
    returned[0] = results[0]

    base = 0
    for part, size in enumerate(PARTS):
        ks = members(part)
        span(results, returned, back_send, back_recv.at[part], ks[0], len(ks)).wait_recv()
        factors = comb[pl.ds(base * SLOTS, size * SLOTS), :].T
        for n in range(0, D, 512):
            rows = returned[pl.ds(base, size), :, n : n + 512].reshape(size * SLOTS, 512)
            both = dot(factors, rows)
            value = acc[:, n : n + 512] + (both[:TOKENS_HERE] + both[TOKENS_HERE:])
            if part < len(PARTS) - 1:
                acc[:, n : n + 512] = value
            else:
                out_ref[:, n : n + 512] = value.astype(BF16)
        base += size

    span(outgoing, arrived, out_send, out_recv.at[0], 1, DEVICES - 1).wait_send()
    span(results, returned, back_send, back_recv.at[0], 1, DEVICES - 1).wait_send()


def on_device(
    residual, pool_input, group_maps, pool_scale, out_proj, norm_gain,
    shared_gate, shared_up, shared_down, expert_gate, expert_up, expert_down,
    expert_ids, route_score,
):
    any_space = pl.BlockSpec(memory_space=pl.ANY)
    vmem = pltpu.VMEM
    block = (DEVICES, SLOTS, D)
    return pl.pallas_call(
        kernel,
        name="mixer_experts",
        out_shape=jax.ShapeDtypeStruct((TOKENS_HERE, D), BF16),
        in_specs=[any_space] * 14,
        out_specs=pl.BlockSpec(memory_space=pltpu.VMEM),
        scratch_shapes=[
            vmem((TOKENS_HERE, D), BF16),
            vmem((REACH + ROWS, CHANNELS), BF16),
            vmem((GROUPS, GW, GW), BF16),
            vmem((8, 128), F32),
            vmem((2 * CHANNELS, D), BF16),
            vmem((D // 128, 128), F32),
            vmem((D, HID), BF16),
            vmem((D, HID), BF16),
            vmem((HID, D), BF16),
            vmem((D, HID), BF16),
            vmem((D, HID), BF16),
            vmem((HID, D), BF16),
            vmem((TOPK, TOKENS_HERE), jnp.int32),
            vmem((TOPK, TOKENS_HERE), F32),
            vmem((ROWS, CHANNELS), BF16),
            vmem((TOKENS_HERE, CHANNELS), BF16),
            vmem((TOKENS_HERE, D), BF16),
            vmem((TOKENS_HERE, D), BF16),
            vmem((TOKENS_HERE, D), F32),
            vmem((DEVICES * SLOTS, TOKENS_HERE), BF16),
            vmem((DEVICES * SLOTS, 2 * TOKENS_HERE), BF16),
            vmem(block, BF16),
            vmem(block, BF16),
            vmem(block, BF16),
            vmem(block, BF16),
            pltpu.SemaphoreType.DMA((14,)),
            pltpu.SemaphoreType.DMA,
            pltpu.SemaphoreType.DMA,
            pltpu.SemaphoreType.DMA,
            pltpu.SemaphoreType.DMA,
            pltpu.SemaphoreType.DMA,
            pltpu.SemaphoreType.DMA((len(PARTS),)),
            pltpu.SemaphoreType.DMA,
            pltpu.SemaphoreType.DMA((len(PARTS),)),
            pltpu.SemaphoreType.REGULAR,
            pltpu.SemaphoreType.REGULAR,
        ],
        compiler_params=pltpu.CompilerParams(
            collective_id=0, has_side_effects=True, vmem_limit_bytes=60 << 20
        ),
    )(
        residual, pool_input, group_maps, pool_scale.reshape(8, 128), out_proj,
        norm_gain.reshape(D // 128, 128), shared_gate, shared_up, shared_down,
        expert_gate, expert_up, expert_down, expert_ids.T, route_score.T,
    )


def solution(mesh):
    in_specs = (
        P(("sp", "tp"), None),
        P("sp", "tp"),
        P(), P(), P(), P(), P(), P(), P(),
        P(("sp", "tp"), None, None),
        P(("sp", "tp"), None, None),
        P(("sp", "tp"), None, None),
        P(("sp", "tp"), None),
        P(("sp", "tp"), None),
    )
    return jax.shard_map(
        on_device, mesh=mesh, in_specs=in_specs, out_specs=P(("sp", "tp"), None), check_vma=False
    )
```

```python
import functools

import jax
import jax.numpy as jnp
from jax import lax
from jax.experimental import pallas as pl
from jax.experimental.pallas import tpu as pltpu
from jax.sharding import PartitionSpec as P

windows = (2, 4, 8, 16)
epsilon = 1e-06
routed_scale = 2.5

MESH = pl.DeviceIdType.MESH
F32 = jnp.float32
BF16 = jnp.bfloat16

SIDE = 4
DEVICES = 128
TOKENS_HERE = 128
TOPK = 4
CAP = 6
SLOTS = 8
D = 2048
HID = 512
ROWS = 256
CHANNELS = 512
GROUPS = 4
GW = 128
REACH = 16
STRIDE = 53
PARTS = (16, 16, 32, 32, 16, 16)


def members(part):
    first = sum(PARTS[:part])
    return range(max(first, 1), first + PARTS[part])


def dot(a, b):
    return jnp.dot(a, b, preferred_element_type=F32)


def offset_of(k):
    kk = k * STRIDE % DEVICES
    return kk // 32, kk // 8 % SIDE, kk // 2 % SIDE, kk % 2


class Place:
    def __init__(self):
        self.sp = lax.axis_index("sp")
        self.tp = lax.axis_index("tp")
        z, y, x = self.sp // 16, self.sp // SIDE % SIDE, self.sp % SIDE
        self.z = [(z + d) % SIDE * 16 for d in range(SIDE)]
        self.y = [(y + d) % SIDE * SIDE for d in range(SIDE)]
        self.x = [(x + d) % SIDE for d in range(SIDE)]
        self.c = [self.tp, 1 - self.tp]

    def at(self, dz, dy, dx, dc):
        return self.z[dz % SIDE] + self.y[dy % SIDE] + self.x[dx % SIDE], self.c[dc]

    def peer(self, k, sign):
        dz, dy, dx, dc = offset_of(k)
        return self.at(sign * dz, sign * dy, sign * dx, dc)


def kernel(
    res_hbm, pool_hbm, maps_hbm, scale_hbm, proj_hbm, gain_hbm,
    sg_hbm, su_hbm, sd_hbm, eg_hbm, eu_hbm, ed_hbm, ids_hbm, score_hbm,
    out_ref,
    res, ext, maps, scale, proj, gain, sg, su, sd, eg, eu, ed, ids, score,
    mix, other_ext, halo, settled, normed, acc, place, comb,
    outgoing, arrived, results, returned,
    in_sems, halo_send, halo_recv, swap_send, swap_recv,
    out_send, out_recv, back_send, back_recv, plane_sem, cube_sem,
):
    here = Place()
    sp, tp = here.sp, here.tp

    barrier = pltpu.get_barrier_semaphore()
    near = [here.at(0, 0, d // 2, d % 2) for d in range(1, 2 * SIDE)]
    near += [here.at(0, d, 0, 0) for d in range(1, SIDE)]
    near += [here.at(d, 0, 0, 0) for d in range(1, SIDE)]
    following = (sp + 1) % (DEVICES // 2)
    previous = (sp + DEVICES // 2 - 1) % (DEVICES // 2)
    near += [(following, 0), (following, 1), (previous, 0), (previous, 1)]
    for device in near:
        pl.semaphore_signal(barrier, inc=1, device_id=device, device_id_type=MESH)

    def fetch(i, src, dst):
        copy = pltpu.make_async_copy(src, dst, in_sems.at[i])
        copy.start()
        return copy

    get_pool = fetch(0, pool_hbm, ext.at[pl.ds(REACH, ROWS)])
    get_ids = fetch(1, ids_hbm, ids)
    get_score = fetch(2, score_hbm, score)
    get_maps = fetch(3, maps_hbm, maps)
    get_scale = fetch(4, scale_hbm, scale)
    get_res = fetch(5, res_hbm, res)
    get_gain = fetch(6, gain_hbm, gain)
    get_proj = fetch(7, proj_hbm, proj)
    ext[:REACH, :] = jnp.zeros((REACH, CHANNELS), BF16)
    pl.semaphore_wait(barrier, len(near))
    for d in range(1, SIDE):
        pl.semaphore_signal(plane_sem, inc=1, device_id=here.at(0, d, 0, 0), device_id_type=MESH)
    get_pool.wait()

    def slab(core):
        return pl.ds(pl.multiple_of(core * TOKENS_HERE, TOKENS_HERE), REACH + TOKENS_HERE)

    swap = pltpu.make_async_remote_copy(
        ext.at[slab(1 - tp)], other_ext, swap_send, swap_recv,
        device_id=(sp, 1 - tp), device_id_type=MESH,
    )
    halos = [
        pltpu.make_async_remote_copy(
            ext.at[pl.ds(ROWS, REACH)], halo.at[i], halo_send.at[i], halo_recv.at[i],
            device_id=(following, [tp, 1 - tp][i]), device_id_type=MESH,
        )
        for i in range(2)
    ]
    halos[0].start()
    halos[1].start()
    swap.start()
    get_sg = fetch(8, sg_hbm, sg)
    get_su = fetch(9, su_hbm, su)
    get_sd = fetch(10, sd_hbm, sd)
    get_eg = fetch(11, eg_hbm.at[0], eg)
    get_eu = fetch(12, eu_hbm.at[0], eu)
    get_ed = fetch(13, ed_hbm.at[0], ed)

    get_ids.wait()
    get_score.wait()
    expert = lax.broadcasted_iota(jnp.int32, (DEVICES, TOKENS_HERE), 0)
    raw = score[...]
    weights = raw / jnp.sum(raw, axis=0, keepdims=True) * routed_scale
    chosen = jnp.zeros((DEVICES, TOKENS_HERE), F32)
    weight = jnp.zeros((DEVICES, TOKENS_HERE), F32)
    for k in range(TOPK):
        hit = expert == ids[k : k + 1, :]
        chosen = jnp.where(hit, 1.0, chosen)
        weight = jnp.where(hit, weights[k : k + 1, :], weight)
    row = lax.broadcasted_iota(jnp.int32, (TOKENS_HERE, TOKENS_HERE), 0)
    column = lax.broadcasted_iota(jnp.int32, (TOKENS_HERE, TOKENS_HERE), 1)
    earlier = (row < column).astype(BF16)
    rank = dot(chosen.astype(BF16), earlier)
    tag = chosen * (rank + 1.0)
    slot_row = lax.broadcasted_iota(jnp.int32, (DEVICES * SLOTS, DEVICES), 0)
    slot_expert = lax.broadcasted_iota(jnp.int32, (DEVICES * SLOTS, DEVICES), 1)
    turn = (slot_row // SLOTS) * STRIDE % DEVICES
    peer_z = (sp // 16 + turn // 32) % SIDE
    peer_y = (sp // SIDE + turn // 8) % SIDE
    peer_x = (sp + turn // 2) % SIDE
    peer = ((peer_z * SIDE + peer_y) * SIDE + peer_x) * 2 + (tp + turn) % 2
    spread = (peer == slot_expert).astype(BF16)
    slot_number = (slot_row % SLOTS + 1).astype(F32)
    place[...] = (dot(spread, tag.astype(BF16)) == slot_number).astype(BF16)
    weight_high = weight.astype(BF16)
    weight_low = (weight - weight_high.astype(F32)).astype(BF16)
    comb[:, :TOKENS_HERE] = dot(spread, weight_high).astype(BF16) * place[...]
    comb[:, TOKENS_HERE:] = dot(spread, weight_low).astype(BF16) * place[...]

    pl.semaphore_wait(plane_sem, SIDE - 1)
    for d in range(1, SIDE):
        pl.semaphore_signal(cube_sem, inc=1, device_id=here.at(d, 0, 0, 0), device_id_type=MESH)

    get_maps.wait()
    get_scale.wait()
    first = sp * ROWS + tp * TOKENS_HERE
    center = lax.broadcasted_iota(jnp.int32, (TOKENS_HERE, REACH + TOKENS_HERE), 0) + REACH
    source = lax.broadcasted_iota(jnp.int32, (TOKENS_HERE, REACH + TOKENS_HERE), 1)
    real = (source >= REACH) | (first > 0)
    position = first + lax.broadcasted_iota(jnp.int32, (TOKENS_HERE, GW), 0)

    def mix_half(i):
        core = [tp, 1 - tp][i]
        rows = ext[slab(tp), :] if i == 0 else other_ext[...]
        head = jnp.where(tp == 0, halo[i].astype(F32), rows[:REACH].astype(F32)).astype(BF16)
        rows = jnp.concatenate([head, rows[REACH:]], axis=0)
        for g in range(GROUPS):
            lanes = slice(g * GW, (g + 1) * GW)
            band = (source <= center) & (source > center - windows[g]) & real
            total = dot(band.astype(BF16), rows[:, lanes])
            divisor = jnp.minimum(position + 1, windows[g]).astype(F32)
            contrast = (total / divisor - rows[REACH:, lanes].astype(F32)).astype(BF16)
            mapped = dot(contrast, maps[core * GROUPS + g])
            low, high = scale[g : g + 1, :], scale[GROUPS + g : GROUPS + g + 1, :]
            mix[:, lanes] = (mapped * jnp.where(core == 0, low, high)).astype(BF16)

    def proj_half(i, n):
        core = [tp, 1 - tp][i]
        part = pl.ds(pl.multiple_of(core * CHANNELS, CHANNELS), CHANNELS)
        return dot(mix[...], proj[part, n : n + 512])

    halos[0].wait()
    mix_half(0)
    get_res.wait()
    get_gain.wait()
    get_proj.wait()
    for n in range(0, D, 512):
        acc[:, n : n + 512] = res[:, n : n + 512].astype(F32) + proj_half(0, n)
    halos[1].wait()
    swap.wait()
    mix_half(1)

    square = jnp.zeros((TOKENS_HERE, 1), F32)
    for n in range(0, D, 512):
        value = (acc[:, n : n + 512] + proj_half(1, n)).astype(BF16)
        settled[:, n : n + 512] = value
        value = value.astype(F32)
        square = square + jnp.sum(value * value, axis=1, keepdims=True)
    inverse = lax.rsqrt(square / D + epsilon)
    for j in range(D // 128):
        lanes = slice(j * 128, (j + 1) * 128)
        value = settled[:, lanes].astype(F32) * inverse * gain[j : j + 1, :]
        normed[:, lanes] = value.astype(BF16)

    base = 0
    for part, size in enumerate(PARTS):
        for n in range(0, D, 512):
            rows = dot(place[pl.ds(base * SLOTS, size * SLOTS), :], normed[:, n : n + 512])
            outgoing[pl.ds(base, size), :, n : n + 512] = rows.astype(BF16).reshape(size, SLOTS, 512)
        base += size
        if part == 0:
            pl.semaphore_wait(cube_sem, SIDE - 1)
        for k in members(part):
            pltpu.make_async_remote_copy(
                outgoing.at[k, pl.ds(0, CAP)], arrived.at[k, pl.ds(0, CAP)],
                out_send, out_recv.at[part],
                device_id=here.peer(k, 1), device_id_type=MESH,
            ).start()
    arrived[0] = outgoing[0]

    def clear(i, _):
        returned[pl.ds(i * 8, 8), CAP:, :] = jnp.zeros((8, SLOTS - CAP, D), BF16)
        return 0

    lax.fori_loop(0, DEVICES // 8, clear, 0)

    get_sg.wait()
    get_su.wait()
    get_sd.wait()
    hidden = dot(normed[...], sg[...])
    hidden = hidden / (1.0 + jnp.exp(-hidden)) * dot(normed[...], su[...])
    hidden = hidden.astype(BF16)
    for n in range(0, D, 512):
        acc[:, n : n + 512] = settled[:, n : n + 512].astype(F32) + dot(hidden, sd[:, n : n + 512])

    get_eg.wait()
    get_eu.wait()
    get_ed.wait()

    def span(src, dst, send_sem, recv_sem, first, count):
        return pltpu.make_async_remote_copy(
            src.at[pl.ds(first, count), pl.ds(0, CAP)], dst.at[pl.ds(first, count), pl.ds(0, CAP)],
            send_sem, recv_sem, device_id=(sp, 1 - tp), device_id_type=MESH,
        )

    base = 0
    for part, size in enumerate(PARTS):
        ks = members(part)
        span(outgoing, arrived, out_send, out_recv.at[part], ks[0], len(ks)).wait_recv()
        rows = arrived[pl.ds(base, size)].reshape(size * SLOTS, D)
        hidden = dot(rows, eg[...])
        hidden = hidden / (1.0 + jnp.exp(-hidden)) * dot(rows, eu[...])
        hidden = hidden.astype(BF16)
        for n in range(0, D, 512):
            value = dot(hidden, ed[:, n : n + 512]).astype(BF16)
            results[pl.ds(base, size), :, n : n + 512] = value.reshape(size, SLOTS, 512)
        for k in ks:
            pltpu.make_async_remote_copy(
                results.at[k, pl.ds(0, CAP)], returned.at[k, pl.ds(0, CAP)],
                back_send, back_recv.at[part],
                device_id=here.peer(k, -1), device_id_type=MESH,
            ).start()
        base += size
    returned[0] = results[0]

    base = 0
    for part, size in enumerate(PARTS):
        ks = members(part)
        span(results, returned, back_send, back_recv.at[part], ks[0], len(ks)).wait_recv()
        factors = comb[pl.ds(base * SLOTS, size * SLOTS), :].T
        for n in range(0, D, 512):
            rows = returned[pl.ds(base, size), :, n : n + 512].reshape(size * SLOTS, 512)
            both = dot(factors, rows)
            value = acc[:, n : n + 512] + (both[:TOKENS_HERE] + both[TOKENS_HERE:])
            if part < len(PARTS) - 1:
                acc[:, n : n + 512] = value
            else:
                out_ref[:, n : n + 512] = value.astype(BF16)
        base += size

    span(outgoing, arrived, out_send, out_recv.at[0], 1, DEVICES - 1).wait_send()
    span(results, returned, back_send, back_recv.at[0], 1, DEVICES - 1).wait_send()


def on_device(
    residual, pool_input, group_maps, pool_scale, out_proj, norm_gain,
    shared_gate, shared_up, shared_down, expert_gate, expert_up, expert_down,
    expert_ids, route_score,
):
    any_space = pl.BlockSpec(memory_space=pl.ANY)
    vmem = pltpu.VMEM
    block = (DEVICES, SLOTS, D)
    return pl.pallas_call(
        kernel,
        name="mixer_experts",
        out_shape=jax.ShapeDtypeStruct((TOKENS_HERE, D), BF16),
        in_specs=[any_space] * 14,
        out_specs=pl.BlockSpec(memory_space=pltpu.VMEM),
        scratch_shapes=[
            vmem((TOKENS_HERE, D), BF16),
            vmem((REACH + ROWS, CHANNELS), BF16),
            vmem((2 * GROUPS, GW, GW), BF16),
            vmem((8, 128), F32),
            vmem((2 * CHANNELS, D), BF16),
            vmem((D // 128, 128), F32),
            vmem((D, HID), BF16),
            vmem((D, HID), BF16),
            vmem((HID, D), BF16),
            vmem((D, HID), BF16),
            vmem((D, HID), BF16),
            vmem((HID, D), BF16),
            vmem((TOPK, TOKENS_HERE), jnp.int32),
            vmem((TOPK, TOKENS_HERE), F32),
            vmem((TOKENS_HERE, CHANNELS), BF16),
            vmem((REACH + TOKENS_HERE, CHANNELS), BF16),
            vmem((2, REACH, CHANNELS), BF16),
            vmem((TOKENS_HERE, D), BF16),
            vmem((TOKENS_HERE, D), BF16),
            vmem((TOKENS_HERE, D), F32),
            vmem((DEVICES * SLOTS, TOKENS_HERE), BF16),
            vmem((DEVICES * SLOTS, 2 * TOKENS_HERE), BF16),
            vmem(block, BF16),
            vmem(block, BF16),
            vmem(block, BF16),
            vmem(block, BF16),
            pltpu.SemaphoreType.DMA((14,)),
            pltpu.SemaphoreType.DMA((2,)),
            pltpu.SemaphoreType.DMA((2,)),
            pltpu.SemaphoreType.DMA,
            pltpu.SemaphoreType.DMA,
            pltpu.SemaphoreType.DMA,
            pltpu.SemaphoreType.DMA((len(PARTS),)),
            pltpu.SemaphoreType.DMA,
            pltpu.SemaphoreType.DMA((len(PARTS),)),
            pltpu.SemaphoreType.REGULAR,
            pltpu.SemaphoreType.REGULAR,
        ],
        compiler_params=pltpu.CompilerParams(
            collective_id=0, has_side_effects=True, vmem_limit_bytes=60 << 20
        ),
    )(
        residual, pool_input, group_maps, pool_scale.reshape(8, 128), out_proj,
        norm_gain.reshape(D // 128, 128), shared_gate, shared_up, shared_down,
        expert_gate, expert_up, expert_down, expert_ids.T, route_score.T,
    )


def solution(mesh):
    in_specs = (
        P(("sp", "tp"), None),
        P("sp", "tp"),
        P(), P(), P(), P(), P(), P(), P(),
        P(("sp", "tp"), None, None),
        P(("sp", "tp"), None, None),
        P(("sp", "tp"), None, None),
        P(("sp", "tp"), None),
        P(("sp", "tp"), None),
    )
    return jax.shard_map(
        on_device, mesh=mesh, in_specs=in_specs, out_specs=P(("sp", "tp"), None), check_vma=False
    )
```

```python
import functools

import jax
import jax.numpy as jnp
from jax import lax
from jax.experimental import pallas as pl
from jax.experimental.pallas import tpu as pltpu
from jax.sharding import PartitionSpec as P

windows = (2, 4, 8, 16)
epsilon = 1e-06
routed_scale = 2.5

MESH = pl.DeviceIdType.MESH
F32 = jnp.float32
BF16 = jnp.bfloat16

SIDE = 4
DEVICES = 128
TOKENS_HERE = 128
TOPK = 4
CAP = 6
SLOTS = 8
D = 2048
HID = 512
ROWS = 256
CHANNELS = 512
GROUPS = 4
GW = 128
REACH = 16
STRIDE = 53
PARTS = (16, 16, 32, 32, 16, 16)


def members(part):
    first = sum(PARTS[:part])
    return range(max(first, 1), first + PARTS[part])


def dot(a, b):
    return jnp.dot(a, b, preferred_element_type=F32)


def offset_of(k):
    kk = k * STRIDE % DEVICES
    return kk // 32, kk // 8 % SIDE, kk // 2 % SIDE, kk % 2


class Place:
    def __init__(self):
        self.sp = lax.axis_index("sp")
        self.tp = lax.axis_index("tp")
        z, y, x = self.sp // 16, self.sp // SIDE % SIDE, self.sp % SIDE
        self.z = [(z + d) % SIDE * 16 for d in range(SIDE)]
        self.y = [(y + d) % SIDE * SIDE for d in range(SIDE)]
        self.x = [(x + d) % SIDE for d in range(SIDE)]
        self.c = [self.tp, 1 - self.tp]

    def at(self, dz, dy, dx, dc):
        return self.z[dz % SIDE] + self.y[dy % SIDE] + self.x[dx % SIDE], self.c[dc]

    def peer(self, k, sign):
        dz, dy, dx, dc = offset_of(k)
        return self.at(sign * dz, sign * dy, sign * dx, dc)


def kernel(
    res_hbm, pool_hbm, maps_hbm, scale_hbm, proj_hbm, gain_hbm,
    sg_hbm, su_hbm, sd_hbm, eg_hbm, eu_hbm, ed_hbm, ids_hbm, score_hbm,
    out_ref,
    res, ext, maps, scale, proj, gain, sg, su, sd, eg, eu, ed, ids, score,
    mix, other_ext, halo, settled, normed, acc, place, comb,
    outgoing, arrived, results, returned,
    in_sems, halo_send, halo_recv, swap_send, swap_recv,
    out_send, out_recv, back_send, back_recv, plane_sem, cube_sem,
):
    here = Place()
    sp, tp = here.sp, here.tp

    barrier = pltpu.get_barrier_semaphore()
    following = (sp + 1) % (DEVICES // 2)
    previous = (sp + DEVICES // 2 - 1) % (DEVICES // 2)
    near = [(sp, 1 - tp), (previous, tp), (previous, 1 - tp), (following, tp), (following, 1 - tp)]
    near += [here.at(0, 0, d // 2, d % 2) for d in range(2, 2 * SIDE)]
    near += [here.at(0, d, 0, 0) for d in range(1, SIDE)]
    near += [here.at(d, 0, 0, 0) for d in range(1, SIDE)]
    for device in near:
        pl.semaphore_signal(barrier, inc=1, device_id=device, device_id_type=MESH)

    def fetch(i, src, dst):
        copy = pltpu.make_async_copy(src, dst, in_sems.at[i])
        copy.start()
        return copy

    get_pool = fetch(0, pool_hbm, ext.at[pl.ds(REACH, ROWS)])
    get_ids = fetch(1, ids_hbm, ids)
    get_score = fetch(2, score_hbm, score)
    get_maps = fetch(3, maps_hbm, maps)
    get_scale = fetch(4, scale_hbm, scale)
    get_res = fetch(5, res_hbm, res)
    get_gain = fetch(6, gain_hbm, gain)
    get_proj = fetch(7, proj_hbm, proj)
    ext[:REACH, :] = jnp.zeros((REACH, CHANNELS), BF16)
    pl.semaphore_wait(barrier, len(near))
    get_pool.wait()

    def slab(core):
        return pl.ds(pl.multiple_of(core * TOKENS_HERE, TOKENS_HERE), REACH + TOKENS_HERE)

    swap = pltpu.make_async_remote_copy(
        ext.at[slab(1 - tp)], other_ext, swap_send, swap_recv,
        device_id=(sp, 1 - tp), device_id_type=MESH,
    )
    halos = [
        pltpu.make_async_remote_copy(
            ext.at[pl.ds(ROWS, REACH)], halo.at[i], halo_send.at[i], halo_recv.at[i],
            device_id=(following, [tp, 1 - tp][i]), device_id_type=MESH,
        )
        for i in range(2)
    ]
    halos[0].start()
    halos[1].start()
    swap.start()
    for d in range(1, SIDE):
        pl.semaphore_signal(plane_sem, inc=1, device_id=here.at(0, d, 0, 0), device_id_type=MESH)
    get_sg = fetch(8, sg_hbm, sg)
    get_su = fetch(9, su_hbm, su)
    get_sd = fetch(10, sd_hbm, sd)
    get_eg = fetch(11, eg_hbm.at[0], eg)
    get_eu = fetch(12, eu_hbm.at[0], eu)
    get_ed = fetch(13, ed_hbm.at[0], ed)

    get_ids.wait()
    get_score.wait()
    expert = lax.broadcasted_iota(jnp.int32, (DEVICES, TOKENS_HERE), 0)
    raw = score[...]
    weights = raw / jnp.sum(raw, axis=0, keepdims=True) * routed_scale
    chosen = jnp.zeros((DEVICES, TOKENS_HERE), F32)
    weight = jnp.zeros((DEVICES, TOKENS_HERE), F32)
    for k in range(TOPK):
        hit = expert == ids[k : k + 1, :]
        chosen = jnp.where(hit, 1.0, chosen)
        weight = jnp.where(hit, weights[k : k + 1, :], weight)
    row = lax.broadcasted_iota(jnp.int32, (TOKENS_HERE, TOKENS_HERE), 0)
    column = lax.broadcasted_iota(jnp.int32, (TOKENS_HERE, TOKENS_HERE), 1)
    earlier = (row < column).astype(BF16)
    rank = dot(chosen.astype(BF16), earlier)
    tag = chosen * (rank + 1.0)
    slot_row = lax.broadcasted_iota(jnp.int32, (DEVICES * SLOTS, DEVICES), 0)
    slot_expert = lax.broadcasted_iota(jnp.int32, (DEVICES * SLOTS, DEVICES), 1)
    turn = (slot_row // SLOTS) * STRIDE % DEVICES
    peer_z = (sp // 16 + turn // 32) % SIDE
    peer_y = (sp // SIDE + turn // 8) % SIDE
    peer_x = (sp + turn // 2) % SIDE
    peer = ((peer_z * SIDE + peer_y) * SIDE + peer_x) * 2 + (tp + turn) % 2
    spread = (peer == slot_expert).astype(BF16)
    slot_number = (slot_row % SLOTS + 1).astype(F32)
    place[...] = (dot(spread, tag.astype(BF16)) == slot_number).astype(BF16)
    weight_high = weight.astype(BF16)
    weight_low = (weight - weight_high.astype(F32)).astype(BF16)
    comb[:, :TOKENS_HERE] = dot(spread, weight_high).astype(BF16) * place[...]
    comb[:, TOKENS_HERE:] = dot(spread, weight_low).astype(BF16) * place[...]

    pl.semaphore_wait(plane_sem, SIDE - 1)
    for d in range(1, SIDE):
        pl.semaphore_signal(cube_sem, inc=1, device_id=here.at(d, 0, 0, 0), device_id_type=MESH)

    get_maps.wait()
    get_scale.wait()
    first = sp * ROWS + tp * TOKENS_HERE
    center = lax.broadcasted_iota(jnp.int32, (TOKENS_HERE, REACH + TOKENS_HERE), 0) + REACH
    source = lax.broadcasted_iota(jnp.int32, (TOKENS_HERE, REACH + TOKENS_HERE), 1)
    real = (source >= REACH) | (first > 0)
    position = first + lax.broadcasted_iota(jnp.int32, (TOKENS_HERE, GW), 0)

    def mix_half(i):
        core = [tp, 1 - tp][i]
        rows = ext[slab(tp), :] if i == 0 else other_ext[...]
        head = jnp.where(tp == 0, halo[i].astype(F32), rows[:REACH].astype(F32)).astype(BF16)
        rows = jnp.concatenate([head, rows[REACH:]], axis=0)
        for g in range(GROUPS):
            lanes = slice(g * GW, (g + 1) * GW)
            band = (source <= center) & (source > center - windows[g]) & real
            total = dot(band.astype(BF16), rows[:, lanes])
            divisor = jnp.minimum(position + 1, windows[g]).astype(F32)
            contrast = (total / divisor - rows[REACH:, lanes].astype(F32)).astype(BF16)
            mapped = dot(contrast, maps[core * GROUPS + g])
            low, high = scale[g : g + 1, :], scale[GROUPS + g : GROUPS + g + 1, :]
            mix[:, lanes] = (mapped * jnp.where(core == 0, low, high)).astype(BF16)

    def proj_half(i, n):
        core = [tp, 1 - tp][i]
        part = pl.ds(pl.multiple_of(core * CHANNELS, CHANNELS), CHANNELS)
        return dot(mix[...], proj[part, n : n + 512])

    halos[0].wait()
    mix_half(0)
    get_res.wait()
    get_gain.wait()
    get_proj.wait()
    for n in range(0, D, 512):
        acc[:, n : n + 512] = res[:, n : n + 512].astype(F32) + proj_half(0, n)
    halos[1].wait()
    swap.wait()
    mix_half(1)

    square = jnp.zeros((TOKENS_HERE, 1), F32)
    for n in range(0, D, 512):
        value = (acc[:, n : n + 512] + proj_half(1, n)).astype(BF16)
        settled[:, n : n + 512] = value
        value = value.astype(F32)
        square = square + jnp.sum(value * value, axis=1, keepdims=True)
    inverse = lax.rsqrt(square / D + epsilon)
    for j in range(D // 128):
        lanes = slice(j * 128, (j + 1) * 128)
        value = settled[:, lanes].astype(F32) * inverse * gain[j : j + 1, :]
        normed[:, lanes] = value.astype(BF16)

    base = 0
    for part, size in enumerate(PARTS):
        for n in range(0, D, 512):
            rows = dot(place[pl.ds(base * SLOTS, size * SLOTS), :], normed[:, n : n + 512])
            outgoing[pl.ds(base, size), :, n : n + 512] = rows.astype(BF16).reshape(size, SLOTS, 512)
        base += size
        if part == 0:
            pl.semaphore_wait(cube_sem, SIDE - 1)
        for k in members(part):
            pltpu.make_async_remote_copy(
                outgoing.at[k, pl.ds(0, CAP)], arrived.at[k, pl.ds(0, CAP)],
                out_send, out_recv.at[part],
                device_id=here.peer(k, 1), device_id_type=MESH,
            ).start()
    arrived[0] = outgoing[0]

    def clear(i, _):
        returned[pl.ds(i * 8, 8), CAP:, :] = jnp.zeros((8, SLOTS - CAP, D), BF16)
        return 0

    lax.fori_loop(0, DEVICES // 8, clear, 0)

    get_sg.wait()
    get_su.wait()
    get_sd.wait()
    hidden = dot(normed[...], sg[...])
    hidden = hidden / (1.0 + jnp.exp(-hidden)) * dot(normed[...], su[...])
    hidden = hidden.astype(BF16)
    for n in range(0, D, 512):
        acc[:, n : n + 512] = settled[:, n : n + 512].astype(F32) + dot(hidden, sd[:, n : n + 512])

    get_eg.wait()
    get_eu.wait()
    get_ed.wait()

    def span(src, dst, send_sem, recv_sem, first, count):
        return pltpu.make_async_remote_copy(
            src.at[pl.ds(first, count), pl.ds(0, CAP)], dst.at[pl.ds(first, count), pl.ds(0, CAP)],
            send_sem, recv_sem, device_id=(sp, 1 - tp), device_id_type=MESH,
        )

    base = 0
    for part, size in enumerate(PARTS):
        ks = members(part)
        span(outgoing, arrived, out_send, out_recv.at[part], ks[0], len(ks)).wait_recv()
        rows = arrived[pl.ds(base, size)].reshape(size * SLOTS, D)
        hidden = dot(rows, eg[...])
        hidden = hidden / (1.0 + jnp.exp(-hidden)) * dot(rows, eu[...])
        hidden = hidden.astype(BF16)
        for n in range(0, D, 512):
            value = dot(hidden, ed[:, n : n + 512]).astype(BF16)
            results[pl.ds(base, size), :, n : n + 512] = value.reshape(size, SLOTS, 512)
        for k in ks:
            pltpu.make_async_remote_copy(
                results.at[k, pl.ds(0, CAP)], returned.at[k, pl.ds(0, CAP)],
                back_send, back_recv.at[part],
                device_id=here.peer(k, -1), device_id_type=MESH,
            ).start()
        base += size
    returned[0] = results[0]

    base = 0
    for part, size in enumerate(PARTS):
        ks = members(part)
        span(results, returned, back_send, back_recv.at[part], ks[0], len(ks)).wait_recv()
        factors = comb[pl.ds(base * SLOTS, size * SLOTS), :].T
        for n in range(0, D, 512):
            rows = returned[pl.ds(base, size), :, n : n + 512].reshape(size * SLOTS, 512)
            both = dot(factors, rows)
            value = acc[:, n : n + 512] + (both[:TOKENS_HERE] + both[TOKENS_HERE:])
            if part < len(PARTS) - 1:
                acc[:, n : n + 512] = value
            else:
                out_ref[:, n : n + 512] = value.astype(BF16)
        base += size

    span(outgoing, arrived, out_send, out_recv.at[0], 1, DEVICES - 1).wait_send()
    span(results, returned, back_send, back_recv.at[0], 1, DEVICES - 1).wait_send()


def on_device(
    residual, pool_input, group_maps, pool_scale, out_proj, norm_gain,
    shared_gate, shared_up, shared_down, expert_gate, expert_up, expert_down,
    expert_ids, route_score,
):
    any_space = pl.BlockSpec(memory_space=pl.ANY)
    vmem = pltpu.VMEM
    block = (DEVICES, SLOTS, D)
    return pl.pallas_call(
        kernel,
        name="mixer_experts",
        out_shape=pltpu.VMEM((TOKENS_HERE, D), BF16),
        in_specs=[any_space] * 14,
        out_specs=pl.BlockSpec(memory_space=pltpu.VMEM),
        scratch_shapes=[
            vmem((TOKENS_HERE, D), BF16),
            vmem((REACH + ROWS, CHANNELS), BF16),
            vmem((2 * GROUPS, GW, GW), BF16),
            vmem((8, 128), F32),
            vmem((2 * CHANNELS, D), BF16),
            vmem((D // 128, 128), F32),
            vmem((D, HID), BF16),
            vmem((D, HID), BF16),
            vmem((HID, D), BF16),
            vmem((D, HID), BF16),
            vmem((D, HID), BF16),
            vmem((HID, D), BF16),
            vmem((TOPK, TOKENS_HERE), jnp.int32),
            vmem((TOPK, TOKENS_HERE), F32),
            vmem((TOKENS_HERE, CHANNELS), BF16),
            vmem((REACH + TOKENS_HERE, CHANNELS), BF16),
            vmem((2, REACH, CHANNELS), BF16),
            vmem((TOKENS_HERE, D), BF16),
            vmem((TOKENS_HERE, D), BF16),
            vmem((TOKENS_HERE, D), F32),
            vmem((DEVICES * SLOTS, TOKENS_HERE), BF16),
            vmem((DEVICES * SLOTS, 2 * TOKENS_HERE), BF16),
            vmem(block, BF16),
            vmem(block, BF16),
            vmem(block, BF16),
            vmem(block, BF16),
            pltpu.SemaphoreType.DMA((14,)),
            pltpu.SemaphoreType.DMA((2,)),
            pltpu.SemaphoreType.DMA((2,)),
            pltpu.SemaphoreType.DMA,
            pltpu.SemaphoreType.DMA,
            pltpu.SemaphoreType.DMA,
            pltpu.SemaphoreType.DMA((len(PARTS),)),
            pltpu.SemaphoreType.DMA,
            pltpu.SemaphoreType.DMA((len(PARTS),)),
            pltpu.SemaphoreType.REGULAR,
            pltpu.SemaphoreType.REGULAR,
        ],
        compiler_params=pltpu.CompilerParams(
            collective_id=0, has_side_effects=True, vmem_limit_bytes=60 << 20
        ),
    )(
        residual, pool_input, group_maps, pool_scale.reshape(8, 128), out_proj,
        norm_gain.reshape(D // 128, 128), shared_gate, shared_up, shared_down,
        expert_gate, expert_up, expert_down, expert_ids.T, route_score.T,
    )


def solution(mesh):
    in_specs = (
        P(("sp", "tp"), None),
        P("sp", "tp"),
        P(), P(), P(), P(), P(), P(), P(),
        P(("sp", "tp"), None, None),
        P(("sp", "tp"), None, None),
        P(("sp", "tp"), None, None),
        P(("sp", "tp"), None),
        P(("sp", "tp"), None),
    )
    return jax.shard_map(
        on_device, mesh=mesh, in_specs=in_specs, out_specs=P(("sp", "tp"), None), check_vma=False
    )
```

```python
import functools

import jax
import jax.numpy as jnp
from jax import lax
from jax.experimental import pallas as pl
from jax.experimental.pallas import tpu as pltpu
from jax.sharding import PartitionSpec as P

windows = (2, 4, 8, 16)
epsilon = 1e-06
routed_scale = 2.5

MESH = pl.DeviceIdType.MESH
F32 = jnp.float32
BF16 = jnp.bfloat16

SIDE = 4
DEVICES = 128
TOKENS_HERE = 128
TOPK = 4
CAP = 6
SLOTS = 8
D = 2048
HID = 512
ROWS = 256
CHANNELS = 512
GROUPS = 4
GW = 128
REACH = 16
STRIDE = 37
ORDERS = 3
COLUMNS = ((0, 640), (640, 640), (1280, 768))
WIDEST = 768
RINGS = 32 * SLOTS
OFFSETS = (0, 1, 3, 2)
WAVES = (1, 0)


def boxes(a, dc):
    every, others = pl.ds(0, SIDE), pl.ds(1, SIDE - 1)
    if dc:
        return [(every, every, every, 1)]
    if a == 0:
        return [(others, every, every, 0), (0, others, every, 0)]
    if a == 1:
        return [(others, every, every, 0), (0, every, others, 0)]
    return [(every, others, every, 0), (every, 0, others, 0)]


def back_boxes(dc):
    every, others = pl.ds(0, SIDE), pl.ds(1, SIDE - 1)
    if dc:
        return [(every, every, every, 1)]
    return [(others, every, every, 0), (0, others, every, 0), (0, 0, others, 0)]


def box_id(a, dc, i):
    return 3 * a + (2 if dc else i)


def back_id(dc, i):
    return 3 if dc else i


def back_spots(dc):
    for n in range(DEVICES // 2):
        k = n * STRIDE % (DEVICES // 2)
        spot = k // 16, k // 4 % SIDE, k % SIDE
        if dc or any(spot):
            yield spot, 0 if spot[0] else 1 if spot[1] else 2


def dot(a, b):
    return jnp.dot(a, b, preferred_element_type=F32)


class Place:
    def __init__(self):
        self.sp = lax.axis_index("sp")
        self.tp = lax.axis_index("tp")
        z, y, x = self.sp // 16, self.sp // SIDE % SIDE, self.sp % SIDE
        self.z = [(z + d) % SIDE * 16 for d in range(SIDE)]
        self.y = [(y + d) % SIDE * SIDE for d in range(SIDE)]
        self.x = [(x + d) % SIDE for d in range(SIDE)]
        self.c = [self.tp, 1 - self.tp]

    def at(self, dz, dy, dx, dc):
        return self.z[dz % SIDE] + self.y[dy % SIDE] + self.x[dx % SIDE], self.c[dc]

    def along(self, a, d):
        return self.at(*[(0, 0, d), (0, d, 0), (d, 0, 0)][a], 0)

    def spot(self, p, u, v, dc, sign):
        return self.at(sign * OFFSETS[p], sign * OFFSETS[u], sign * OFFSETS[v], dc)


def kernel(
    res_hbm, pool_hbm, maps_hbm, scale_hbm, proj_hbm, gain_hbm,
    sg_hbm, su_hbm, sd_hbm, eg_hbm, eu_hbm, ed_hbm, ids_hbm, score_hbm,
    out_ref,
    res, ext, maps, scale, proj, gain, sg, su, sd, eg, eu, ed, ids, score,
    mix, other_ext, halo, settled, normed, acc,
    ring_ids, place, comb, ring_rows,
    outgoing, arrived, results, returned,
    in_sems, halo_send, halo_recv, swap_send, swap_recv,
    table_send, table_recv, ring_send, ring_recv, far_send, far_recv,
    out_send, out_recv, back_send, back_recv, plane_sem, cube_sem,
):
    here = Place()
    sp, tp = here.sp, here.tp

    barrier = pltpu.get_barrier_semaphore()
    following = (sp + 1) % (DEVICES // 2)
    previous = (sp + DEVICES // 2 - 1) % (DEVICES // 2)
    near = [(sp, 1 - tp), (previous, tp), (previous, 1 - tp), (following, tp), (following, 1 - tp)]
    near += [here.at(0, 0, d // 2, d % 2) for d in range(2, 2 * SIDE)]
    near += [here.at(0, d, 0, 0) for d in range(1, SIDE)]
    near += [here.at(d, 0, 0, 0) for d in range(1, SIDE)]
    for device in near:
        pl.semaphore_signal(barrier, inc=1, device_id=device, device_id_type=MESH)

    def fetch(i, src, dst):
        copy = pltpu.make_async_copy(src, dst, in_sems.at[i])
        copy.start()
        return copy

    get_pool = fetch(0, pool_hbm, ext.at[pl.ds(REACH, ROWS)])
    get_ids = fetch(1, ids_hbm, ids)
    get_score = fetch(2, score_hbm, score)
    get_maps = fetch(3, maps_hbm, maps)
    get_scale = fetch(4, scale_hbm, scale)
    get_res = fetch(5, res_hbm, res)
    get_gain = fetch(6, gain_hbm, gain)
    get_proj = fetch(7, proj_hbm, proj)
    ext[:REACH, :] = jnp.zeros((REACH, CHANNELS), BF16)
    pl.semaphore_wait(barrier, len(near))
    get_pool.wait()

    def slab(core):
        return pl.ds(pl.multiple_of(core * TOKENS_HERE, TOKENS_HERE), REACH + TOKENS_HERE)

    swap = pltpu.make_async_remote_copy(
        ext.at[slab(1 - tp)], other_ext, swap_send, swap_recv,
        device_id=(sp, 1 - tp), device_id_type=MESH,
    )
    halos = [
        pltpu.make_async_remote_copy(
            ext.at[pl.ds(ROWS, REACH)], halo.at[i], halo_send.at[i], halo_recv.at[i],
            device_id=(following, [tp, 1 - tp][i]), device_id_type=MESH,
        )
        for i in range(2)
    ]
    halos[0].start()
    halos[1].start()
    swap.start()
    for d in range(1, SIDE):
        pl.semaphore_signal(plane_sem, inc=1, device_id=here.at(0, d, 0, 0), device_id_type=MESH)
    get_sg = fetch(8, sg_hbm, sg)
    get_su = fetch(9, su_hbm, su)
    get_sd = fetch(10, sd_hbm, sd)
    get_eg = fetch(11, eg_hbm.at[0], eg)
    get_eu = fetch(12, eu_hbm.at[0], eu)
    get_ed = fetch(13, ed_hbm.at[0], ed)

    get_ids.wait()
    get_score.wait()
    for a in range(ORDERS):
        for j in range(1, SIDE):
            pltpu.make_async_remote_copy(
                ids, ring_ids.at[a, j], table_send, table_recv,
                device_id=here.along(a, OFFSETS[j]), device_id_type=MESH,
            ).start()

    expert = lax.broadcasted_iota(jnp.int32, (DEVICES, TOKENS_HERE), 0)
    before = lax.broadcasted_iota(jnp.int32, (TOKENS_HERE, TOKENS_HERE), 0)
    token = lax.broadcasted_iota(jnp.int32, (TOKENS_HERE, TOKENS_HERE), 1)
    earlier = (before < token).astype(BF16)
    slot_row = lax.broadcasted_iota(jnp.int32, (RINGS, DEVICES), 0)
    slot_expert = lax.broadcasted_iota(jnp.int32, (RINGS, DEVICES), 1)
    slot_number = (slot_row % SLOTS + 1).astype(F32)
    u, v, c = slot_row // 64, slot_row // 16 % SIDE, slot_row // 8 % 2
    u, v = jnp.where(u < 2, u, 5 - u), jnp.where(v < 2, v, 5 - v)
    z, y, x = sp // 16, sp // SIDE % SIDE, sp % SIDE
    c = (tp + c) % 2

    def spread_over(chip):
        return (chip * 2 + c == slot_expert).astype(BF16)

    spread = [
        spread_over(((z + u) % SIDE * SIDE + (y + v) % SIDE) * SIDE + x),
        spread_over(((z + u) % SIDE * SIDE + y) * SIDE + (x + v) % SIDE),
        spread_over((z * SIDE + (y + u) % SIDE) * SIDE + (x + v) % SIDE),
    ]

    def tag_of(rows):
        chosen = jnp.zeros((DEVICES, TOKENS_HERE), F32)
        for k in range(TOPK):
            chosen = jnp.where(expert == rows[k : k + 1, :], 1.0, chosen)
        return (chosen * (dot(chosen.astype(BF16), earlier) + 1.0)).astype(BF16)

    def set_place(a, j, tag):
        place[a * SIDE + j] = (dot(spread[a], tag) == slot_number).astype(BF16)

    own_tag = tag_of(ids[...])
    for a in range(ORDERS):
        set_place(a, 0, own_tag)

    pl.semaphore_wait(plane_sem, SIDE - 1)
    for d in range(1, SIDE):
        pl.semaphore_signal(cube_sem, inc=1, device_id=here.at(d, 0, 0, 0), device_id_type=MESH)

    get_maps.wait()
    get_scale.wait()
    first = sp * ROWS + tp * TOKENS_HERE
    center = lax.broadcasted_iota(jnp.int32, (TOKENS_HERE, REACH + TOKENS_HERE), 0) + REACH
    source = lax.broadcasted_iota(jnp.int32, (TOKENS_HERE, REACH + TOKENS_HERE), 1)
    real = (source >= REACH) | (first > 0)
    position = first + lax.broadcasted_iota(jnp.int32, (TOKENS_HERE, GW), 0)

    def mix_half(i):
        core = [tp, 1 - tp][i]
        rows = ext[slab(tp), :] if i == 0 else other_ext[...]
        head = jnp.where(tp == 0, halo[i].astype(F32), rows[:REACH].astype(F32)).astype(BF16)
        rows = jnp.concatenate([head, rows[REACH:]], axis=0)
        for g in range(GROUPS):
            lanes = slice(g * GW, (g + 1) * GW)
            band = (source <= center) & (source > center - windows[g]) & real
            total = dot(band.astype(BF16), rows[:, lanes])
            divisor = jnp.minimum(position + 1, windows[g]).astype(F32)
            contrast = (total / divisor - rows[REACH:, lanes].astype(F32)).astype(BF16)
            mapped = dot(contrast, maps[core * GROUPS + g])
            low, high = scale[g : g + 1, :], scale[GROUPS + g : GROUPS + g + 1, :]
            mix[:, lanes] = (mapped * jnp.where(core == 0, low, high)).astype(BF16)

    def proj_half(i, n):
        core = [tp, 1 - tp][i]
        part = pl.ds(pl.multiple_of(core * CHANNELS, CHANNELS), CHANNELS)
        return dot(mix[...], proj[part, n : n + 512])

    halos[0].wait()
    mix_half(0)
    get_res.wait()
    get_gain.wait()
    get_proj.wait()
    for n in range(0, D, 512):
        acc[:, n : n + 512] = res[:, n : n + 512].astype(F32) + proj_half(0, n)
    halos[1].wait()
    swap.wait()
    mix_half(1)

    square = jnp.zeros((TOKENS_HERE, 1), F32)
    for n in range(0, D, 512):
        value = (acc[:, n : n + 512] + proj_half(1, n)).astype(BF16)
        settled[:, n : n + 512] = value
        value = value.astype(F32)
        square = square + jnp.sum(value * value, axis=1, keepdims=True)
    inverse = lax.rsqrt(square / D + epsilon)
    for j in range(D // 128):
        lanes = slice(j * 128, (j + 1) * 128)
        value = settled[:, lanes].astype(F32) * inverse * gain[j : j + 1, :]
        normed[:, lanes] = value.astype(BF16)

    def ring(a, j):
        first, width = COLUMNS[a]
        return pltpu.make_async_remote_copy(
            normed.at[:, pl.ds(first, width)], ring_rows.at[a, j, :, pl.ds(0, width)],
            ring_send.at[a, j], ring_recv.at[a, j],
            device_id=here.along(a, OFFSETS[j]), device_id_type=MESH,
        )

    def onward(a, j):
        half = pl.ds((j - 1) * (TOKENS_HERE // 2), TOKENS_HERE // 2)
        part = pl.ds(0, COLUMNS[a][1])
        return pltpu.make_async_remote_copy(
            ring_rows.at[a, j, half, part], ring_rows.at[a, 3, half, part],
            far_send.at[a, j], far_recv.at[a, j],
            device_id=here.along(a, OFFSETS[j]), device_id_type=MESH,
        )

    for j in (1, 2):
        for a in range(ORDERS):
            ring(a, j).start()

    def block(ref, index, a):
        first, width = COLUMNS[a]
        return ref.at[(*index, pl.ds(0, CAP), pl.ds(first, width))]

    def ship(dc, lead):
        for u in range(SIDE):
            for v in range(SIDE):
                if u or v or dc:
                    for a in range(ORDERS):
                        spot = [(u, v, 0), (u, 0, v), (0, u, v)][a]
                        index = [(u, v, lead), (u, lead, v), (lead, u, v)][a]
                        sem = box_id(a, dc, 0 if u else 1)
                        pltpu.make_async_remote_copy(
                            block(outgoing, (*index, dc), a), block(arrived, (*index, dc), a),
                            out_send.at[sem], out_recv.at[sem],
                            device_id=here.spot(*spot, dc, 1), device_id_type=MESH,
                        ).start()

    def plane(a, j):
        first, width = COLUMNS[a]
        every, columns = slice(None), slice(first, first + width)
        lead = [(every, every, j), (every, j, every), (j, every, every)][a]
        return (*lead, every, every, columns)

    def local(a):
        first, width = COLUMNS[a]
        every, columns = slice(None), slice(first, first + width)
        lead = [(0, 0, every, 0), (0, every, 0, 0), (every, 0, 0, 0)][a]
        return (*lead, every, columns)

    def fill(a, j, rows):
        value = dot(place[a * SIDE + j], rows).astype(BF16)
        outgoing[plane(a, j)] = value.reshape(SIDE, SIDE, 2, SLOTS, COLUMNS[a][1])

    for a, (first, width) in enumerate(COLUMNS):
        fill(a, 0, normed[:, first : first + width])
    pl.semaphore_wait(cube_sem, SIDE - 1)
    for dc in WAVES:
        ship(dc, 0)

    others = pl.ds(1, SIDE - 1)
    pltpu.make_async_remote_copy(
        ring_ids.at[:, others], ring_ids.at[:, others], table_send, table_recv,
        device_id=(sp, 1 - tp), device_id_type=MESH,
    ).wait()
    for a in range(ORDERS):
        for j in (1, 2):
            set_place(a, j, tag_of(ring_ids[a, j]))
    for j in (1, 2):
        for a in range(ORDERS):
            ring(a, j).wait_recv()
            onward(a, j).start()
    for j in (1, 2):
        for a in range(ORDERS):
            fill(a, j, ring_rows[a, j, :, : COLUMNS[a][1]])
    ship(WAVES[0], pl.ds(1, 2))
    for a in range(ORDERS):
        set_place(a, 3, tag_of(ring_ids[a, 3]))
    for a in range(ORDERS):
        onward(a, 1).wait_recv()
        onward(a, 2).wait_recv()
        fill(a, 3, ring_rows[a, 3, :, : COLUMNS[a][1]])
    ship(WAVES[0], 3)
    ship(WAVES[1], pl.ds(1, 2))
    ship(WAVES[1], 3)
    for a in range(ORDERS):
        arrived[local(a)] = outgoing[local(a)]

    def clear(i, _):
        returned[i // SIDE, i % SIDE, :, :, CAP:, :] = jnp.zeros((SIDE, 2, SLOTS - CAP, D), BF16)
        return 0

    lax.fori_loop(0, SIDE * SIDE, clear, 0)

    get_sg.wait()
    get_su.wait()
    get_sd.wait()
    hidden = dot(normed[...], sg[...])
    hidden = hidden / (1.0 + jnp.exp(-hidden)) * dot(normed[...], su[...])
    hidden = hidden.astype(BF16)
    for n in range(0, D, 512):
        acc[:, n : n + 512] = settled[:, n : n + 512].astype(F32) + dot(hidden, sd[:, n : n + 512])

    get_eg.wait()
    get_eu.wait()
    get_ed.wait()

    raw = score[...]
    weights = raw / jnp.sum(raw, axis=0, keepdims=True) * routed_scale
    weight = jnp.zeros((DEVICES, TOKENS_HERE), F32)
    for k in range(TOPK):
        weight = jnp.where(expert == ids[k : k + 1, :], weights[k : k + 1, :], weight)
    high = weight.astype(BF16)
    low = (weight - high.astype(F32)).astype(BF16)
    slot_row = lax.broadcasted_iota(jnp.int32, (2 * RINGS, DEVICES), 0)
    slot_expert = lax.broadcasted_iota(jnp.int32, (2 * RINGS, DEVICES), 1)
    slot_number = (slot_row % SLOTS + 1).astype(F32)
    w, u, v = slot_row // 128, slot_row // 32 % SIDE, slot_row // 8 % SIDE
    w, u, v = [jnp.where(i < 2, i, 5 - i) for i in (w, u, v)]
    chip = ((z + w) % SIDE * SIDE + (y + u) % SIDE) * SIDE + (x + v) % SIDE
    for dc in range(2):
        over = (chip * 2 + (tp + dc) % 2 == slot_expert).astype(BF16)
        where = (dot(over, own_tag) == slot_number).astype(F32)
        comb[dc, :TOKENS_HERE, :] = (dot(over, high) * where).T.astype(BF16)
        comb[dc, TOKENS_HERE:, :] = (dot(over, low) * where).T.astype(BF16)

    def box(a, dc, i):
        index, sem = boxes(a, dc)[i], box_id(a, dc, i)
        return pltpu.make_async_remote_copy(
            block(outgoing, index, a), block(arrived, index, a), out_send.at[sem], out_recv.at[sem],
            device_id=(sp, 1 - tp), device_id_type=MESH,
        )

    def back_copy(index, sem, device):
        index = (*index, pl.ds(0, CAP))
        return pltpu.make_async_remote_copy(
            results.at[index], returned.at[index], back_send.at[sem], back_recv.at[sem],
            device_id=device, device_id_type=MESH,
        )

    def back_box(dc, i):
        return back_copy(back_boxes(dc)[i], back_id(dc, i), (sp, 1 - tp))

    for dc in WAVES:
        for a in range(ORDERS):
            for i in range(len(boxes(a, dc))):
                box(a, dc, i).wait_recv()
        for p in range(0, SIDE, 2):
            rows = arrived[p : p + 2, :, :, dc].reshape(RINGS, D)
            hidden = dot(rows, eg[...])
            hidden = hidden / (1.0 + jnp.exp(-hidden)) * dot(rows, eu[...])
            hidden = hidden.astype(BF16)
            for n in range(0, D, 512):
                value = dot(hidden, ed[:, n : n + 512]).astype(BF16)
                results[p : p + 2, :, :, dc, :, n : n + 512] = value.reshape(2, SIDE, SIDE, SLOTS, 512)
        for spot, i in back_spots(dc):
            back_copy((*spot, dc), back_id(dc, i), here.spot(*spot, dc, -1)).start()
    returned[0, 0, 0, 0] = results[0, 0, 0, 0]

    for dc in WAVES:
        for i in range(len(back_boxes(dc))):
            back_box(dc, i).wait_recv()
        for n in range(0, D, 512):
            rows = returned[:, :, :, dc, :, n : n + 512].reshape(2 * RINGS, 512)
            both = dot(comb[dc], rows)
            value = acc[:, n : n + 512] + (both[:TOKENS_HERE] + both[TOKENS_HERE:])
            if dc != WAVES[-1]:
                acc[:, n : n + 512] = value
            else:
                out_ref[:, n : n + 512] = value.astype(BF16)

    for dc in range(2):
        for a in range(ORDERS):
            for i in range(len(boxes(a, dc))):
                box(a, dc, i).wait_send()
        for i in range(len(back_boxes(dc))):
            back_box(dc, i).wait_send()
    for a in range(ORDERS):
        for j in (1, 2):
            ring(a, j).wait_send()
            onward(a, j).wait_send()


def on_device(
    residual, pool_input, group_maps, pool_scale, out_proj, norm_gain,
    shared_gate, shared_up, shared_down, expert_gate, expert_up, expert_down,
    expert_ids, route_score,
):
    any_space = pl.BlockSpec(memory_space=pl.ANY)
    vmem = pltpu.VMEM
    block = (SIDE, SIDE, SIDE, 2, SLOTS, D)
    dma = pltpu.SemaphoreType.DMA
    return pl.pallas_call(
        kernel,
        name="mixer_experts",
        out_shape=pltpu.VMEM((TOKENS_HERE, D), BF16),
        in_specs=[any_space] * 14,
        out_specs=pl.BlockSpec(memory_space=pltpu.VMEM),
        scratch_shapes=[
            vmem((TOKENS_HERE, D), BF16),
            vmem((REACH + ROWS, CHANNELS), BF16),
            vmem((2 * GROUPS, GW, GW), BF16),
            vmem((8, 128), F32),
            vmem((2 * CHANNELS, D), BF16),
            vmem((D // 128, 128), F32),
            vmem((D, HID), BF16),
            vmem((D, HID), BF16),
            vmem((HID, D), BF16),
            vmem((D, HID), BF16),
            vmem((D, HID), BF16),
            vmem((HID, D), BF16),
            vmem((TOPK, TOKENS_HERE), jnp.int32),
            vmem((TOPK, TOKENS_HERE), F32),
            vmem((TOKENS_HERE, CHANNELS), BF16),
            vmem((REACH + TOKENS_HERE, CHANNELS), BF16),
            vmem((2, REACH, CHANNELS), BF16),
            vmem((TOKENS_HERE, D), BF16),
            vmem((TOKENS_HERE, D), BF16),
            vmem((TOKENS_HERE, D), F32),
            vmem((ORDERS, SIDE, TOPK, TOKENS_HERE), jnp.int32),
            vmem((ORDERS * SIDE, RINGS, TOKENS_HERE), BF16),
            vmem((2, 2 * TOKENS_HERE, 2 * RINGS), BF16),
            vmem((ORDERS, SIDE, TOKENS_HERE, WIDEST), BF16),
            vmem(block, BF16),
            vmem(block, BF16),
            vmem(block, BF16),
            vmem(block, BF16),
            dma((14,)),
            dma((2,)), dma((2,)), dma, dma,
            dma, dma, dma((ORDERS, SIDE)), dma((ORDERS, SIDE)), dma((ORDERS, SIDE)), dma((ORDERS, SIDE)),
            dma((9,)), dma((9,)), dma((4,)), dma((4,)),
            pltpu.SemaphoreType.REGULAR,
            pltpu.SemaphoreType.REGULAR,
        ],
        compiler_params=pltpu.CompilerParams(
            collective_id=0, has_side_effects=True, vmem_limit_bytes=60 << 20
        ),
    )(
        residual, pool_input, group_maps, pool_scale.reshape(8, 128), out_proj,
        norm_gain.reshape(D // 128, 128), shared_gate, shared_up, shared_down,
        expert_gate, expert_up, expert_down, expert_ids.T, route_score.T,
    )


def solution(mesh):
    in_specs = (
        P(("sp", "tp"), None),
        P("sp", "tp"),
        P(), P(), P(), P(), P(), P(), P(),
        P(("sp", "tp"), None, None),
        P(("sp", "tp"), None, None),
        P(("sp", "tp"), None, None),
        P(("sp", "tp"), None),
        P(("sp", "tp"), None),
    )
    return jax.shard_map(
        on_device, mesh=mesh, in_specs=in_specs, out_specs=P(("sp", "tp"), None), check_vma=False
    )
```

```python
import functools

import jax
import jax.numpy as jnp
from jax import lax
from jax.experimental import pallas as pl
from jax.experimental.pallas import tpu as pltpu
from jax.sharding import PartitionSpec as P

windows = (2, 4, 8, 16)
epsilon = 1e-06
routed_scale = 2.5

MESH = pl.DeviceIdType.MESH
F32 = jnp.float32
BF16 = jnp.bfloat16

SIDE = 4
DEVICES = 128
TOKENS_HERE = 128
TOPK = 4
CAP = 6
SLOTS = 8
D = 2048
HID = 512
ROWS = 256
CHANNELS = 512
GROUPS = 4
GW = 128
REACH = 16
STRIDE = 37
ORDERS = 3
COLUMNS = ((0, 640), (640, 640), (1280, 768))
WIDEST = 768
RINGS = 32 * SLOTS
OFFSETS = (0, 1, 3, 2)
HALVES = (1, 0)
WAVES = (1, 0)


def boxes(a, dc):
    every, others = pl.ds(0, SIDE), pl.ds(1, SIDE - 1)
    if dc:
        return [(every, every, every, 1)]
    if a == 0:
        return [(others, every, every, 0), (0, others, every, 0)]
    if a == 1:
        return [(others, every, every, 0), (0, every, others, 0)]
    return [(every, others, every, 0), (every, 0, others, 0)]


def back_boxes(dc, half):
    every, others, both = pl.ds(0, SIDE), pl.ds(1, SIDE - 1), pl.ds(2 * half, 2)
    if dc or half:
        return [(every, every, both, dc)]
    return [(others, every, both, 0), (0, others, both, 0), (0, 0, 1, 0)]


def box_id(a, dc, i):
    return 3 * a + (2 if dc else i)


def back_id(dc, half, i):
    return 2 + half if dc else 4 if half else i if i < 2 else 5


def back_spots(dc, half):
    for n in range(DEVICES // 2):
        k = n * STRIDE % (DEVICES // 2)
        spot = k // 16, k // 4 % SIDE, k % SIDE
        if spot[2] // 2 == half and (dc or any(spot)):
            yield spot, 0 if dc or half or spot[0] else 1 if spot[1] else 2


def dot(a, b):
    return jnp.dot(a, b, preferred_element_type=F32)


class Place:
    def __init__(self):
        self.sp = lax.axis_index("sp")
        self.tp = lax.axis_index("tp")
        z, y, x = self.sp // 16, self.sp // SIDE % SIDE, self.sp % SIDE
        self.z = [(z + d) % SIDE * 16 for d in range(SIDE)]
        self.y = [(y + d) % SIDE * SIDE for d in range(SIDE)]
        self.x = [(x + d) % SIDE for d in range(SIDE)]
        self.c = [self.tp, 1 - self.tp]

    def at(self, dz, dy, dx, dc):
        return self.z[dz % SIDE] + self.y[dy % SIDE] + self.x[dx % SIDE], self.c[dc]

    def along(self, a, d):
        return self.at(*[(0, 0, d), (0, d, 0), (d, 0, 0)][a], 0)

    def spot(self, p, u, v, dc, sign):
        return self.at(sign * OFFSETS[p], sign * OFFSETS[u], sign * OFFSETS[v], dc)


def kernel(
    res_hbm, pool_hbm, maps_hbm, scale_hbm, proj_hbm, gain_hbm,
    sg_hbm, su_hbm, sd_hbm, eg_hbm, eu_hbm, ed_hbm, ids_hbm, score_hbm,
    out_ref,
    res, ext, maps, scale, proj, gain, sg, su, sd, eg, eu, ed, ids, score,
    mix, other_ext, halo, settled, normed, acc,
    ring_ids, place, comb, ring_rows,
    outgoing, arrived, results, returned,
    in_sems, halo_send, halo_recv, swap_send, swap_recv,
    table_send, table_recv, ring_send, ring_recv, far_send, far_recv,
    out_send, out_recv, back_send, back_recv, plane_sem, cube_sem,
):
    here = Place()
    sp, tp = here.sp, here.tp

    barrier = pltpu.get_barrier_semaphore()
    following = (sp + 1) % (DEVICES // 2)
    previous = (sp + DEVICES // 2 - 1) % (DEVICES // 2)
    near = [(sp, 1 - tp), (previous, tp), (previous, 1 - tp), (following, tp), (following, 1 - tp)]
    near += [here.at(0, 0, d // 2, d % 2) for d in range(2, 2 * SIDE)]
    near += [here.at(0, d, 0, 0) for d in range(1, SIDE)]
    near += [here.at(d, 0, 0, 0) for d in range(1, SIDE)]
    for device in near:
        pl.semaphore_signal(barrier, inc=1, device_id=device, device_id_type=MESH)

    def fetch(i, src, dst):
        copy = pltpu.make_async_copy(src, dst, in_sems.at[i])
        copy.start()
        return copy

    get_pool = fetch(0, pool_hbm, ext.at[pl.ds(REACH, ROWS)])
    get_ids = fetch(1, ids_hbm, ids)
    get_score = fetch(2, score_hbm, score)
    get_maps = fetch(3, maps_hbm, maps)
    get_scale = fetch(4, scale_hbm, scale)
    get_res = fetch(5, res_hbm, res)
    get_gain = fetch(6, gain_hbm, gain)
    get_proj = fetch(7, proj_hbm, proj)
    ext[:REACH, :] = jnp.zeros((REACH, CHANNELS), BF16)
    pl.semaphore_wait(barrier, len(near))
    get_pool.wait()

    def slab(core):
        return pl.ds(pl.multiple_of(core * TOKENS_HERE, TOKENS_HERE), REACH + TOKENS_HERE)

    swap = pltpu.make_async_remote_copy(
        ext.at[slab(1 - tp)], other_ext, swap_send, swap_recv,
        device_id=(sp, 1 - tp), device_id_type=MESH,
    )
    halos = [
        pltpu.make_async_remote_copy(
            ext.at[pl.ds(ROWS, REACH)], halo.at[i], halo_send.at[i], halo_recv.at[i],
            device_id=(following, [tp, 1 - tp][i]), device_id_type=MESH,
        )
        for i in range(2)
    ]
    halos[0].start()
    halos[1].start()
    swap.start()
    for d in range(1, SIDE):
        pl.semaphore_signal(plane_sem, inc=1, device_id=here.at(0, d, 0, 0), device_id_type=MESH)
    get_sg = fetch(8, sg_hbm, sg)
    get_su = fetch(9, su_hbm, su)
    get_sd = fetch(10, sd_hbm, sd)
    get_eg = fetch(11, eg_hbm.at[0], eg)
    get_eu = fetch(12, eu_hbm.at[0], eu)
    get_ed = fetch(13, ed_hbm.at[0], ed)

    get_ids.wait()
    get_score.wait()
    for a in range(ORDERS):
        for j in range(1, SIDE):
            pltpu.make_async_remote_copy(
                ids, ring_ids.at[a, j], table_send, table_recv,
                device_id=here.along(a, OFFSETS[j]), device_id_type=MESH,
            ).start()

    expert = lax.broadcasted_iota(jnp.int32, (DEVICES, TOKENS_HERE), 0)
    before = lax.broadcasted_iota(jnp.int32, (TOKENS_HERE, TOKENS_HERE), 0)
    token = lax.broadcasted_iota(jnp.int32, (TOKENS_HERE, TOKENS_HERE), 1)
    earlier = (before < token).astype(BF16)
    slot_row = lax.broadcasted_iota(jnp.int32, (RINGS, DEVICES), 0)
    slot_expert = lax.broadcasted_iota(jnp.int32, (RINGS, DEVICES), 1)
    slot_number = (slot_row % SLOTS + 1).astype(F32)
    u, v, c = slot_row // 64, slot_row // 16 % SIDE, slot_row // 8 % 2
    u, v = jnp.where(u < 2, u, 5 - u), jnp.where(v < 2, v, 5 - v)
    z, y, x = sp // 16, sp // SIDE % SIDE, sp % SIDE
    c = (tp + c) % 2

    def spread_over(chip):
        return (chip * 2 + c == slot_expert).astype(BF16)

    spread = [
        spread_over(((z + u) % SIDE * SIDE + (y + v) % SIDE) * SIDE + x),
        spread_over(((z + u) % SIDE * SIDE + y) * SIDE + (x + v) % SIDE),
        spread_over((z * SIDE + (y + u) % SIDE) * SIDE + (x + v) % SIDE),
    ]

    def tag_of(rows):
        chosen = jnp.zeros((DEVICES, TOKENS_HERE), F32)
        for k in range(TOPK):
            chosen = jnp.where(expert == rows[k : k + 1, :], 1.0, chosen)
        return (chosen * (dot(chosen.astype(BF16), earlier) + 1.0)).astype(BF16)

    def set_place(a, j, tag):
        place[a * SIDE + j] = (dot(spread[a], tag) == slot_number).astype(BF16)

    own_tag = tag_of(ids[...])
    for a in range(ORDERS):
        set_place(a, 0, own_tag)

    pl.semaphore_wait(plane_sem, SIDE - 1)
    for d in range(1, SIDE):
        pl.semaphore_signal(cube_sem, inc=1, device_id=here.at(d, 0, 0, 0), device_id_type=MESH)

    get_maps.wait()
    get_scale.wait()
    first = sp * ROWS + tp * TOKENS_HERE
    center = lax.broadcasted_iota(jnp.int32, (TOKENS_HERE, REACH + TOKENS_HERE), 0) + REACH
    source = lax.broadcasted_iota(jnp.int32, (TOKENS_HERE, REACH + TOKENS_HERE), 1)
    real = (source >= REACH) | (first > 0)
    position = first + lax.broadcasted_iota(jnp.int32, (TOKENS_HERE, GW), 0)

    def mix_half(i):
        core = [tp, 1 - tp][i]
        rows = ext[slab(tp), :] if i == 0 else other_ext[...]
        head = jnp.where(tp == 0, halo[i].astype(F32), rows[:REACH].astype(F32)).astype(BF16)
        rows = jnp.concatenate([head, rows[REACH:]], axis=0)
        for g in range(GROUPS):
            lanes = slice(g * GW, (g + 1) * GW)
            band = (source <= center) & (source > center - windows[g]) & real
            total = dot(band.astype(BF16), rows[:, lanes])
            divisor = jnp.minimum(position + 1, windows[g]).astype(F32)
            contrast = (total / divisor - rows[REACH:, lanes].astype(F32)).astype(BF16)
            mapped = dot(contrast, maps[core * GROUPS + g])
            low, high = scale[g : g + 1, :], scale[GROUPS + g : GROUPS + g + 1, :]
            mix[:, lanes] = (mapped * jnp.where(core == 0, low, high)).astype(BF16)

    def proj_half(i, n):
        core = [tp, 1 - tp][i]
        part = pl.ds(pl.multiple_of(core * CHANNELS, CHANNELS), CHANNELS)
        return dot(mix[...], proj[part, n : n + 512])

    halos[0].wait()
    mix_half(0)
    get_res.wait()
    get_gain.wait()
    get_proj.wait()
    for n in range(0, D, 512):
        acc[:, n : n + 512] = res[:, n : n + 512].astype(F32) + proj_half(0, n)
    halos[1].wait()
    swap.wait()
    mix_half(1)

    square = jnp.zeros((TOKENS_HERE, 1), F32)
    for n in range(0, D, 512):
        value = (acc[:, n : n + 512] + proj_half(1, n)).astype(BF16)
        settled[:, n : n + 512] = value
        value = value.astype(F32)
        square = square + jnp.sum(value * value, axis=1, keepdims=True)
    inverse = lax.rsqrt(square / D + epsilon)
    for j in range(D // 128):
        lanes = slice(j * 128, (j + 1) * 128)
        value = settled[:, lanes].astype(F32) * inverse * gain[j : j + 1, :]
        normed[:, lanes] = value.astype(BF16)

    def ring(a, j):
        first, width = COLUMNS[a]
        return pltpu.make_async_remote_copy(
            normed.at[:, pl.ds(first, width)], ring_rows.at[a, j, :, pl.ds(0, width)],
            ring_send.at[a, j], ring_recv.at[a, j],
            device_id=here.along(a, OFFSETS[j]), device_id_type=MESH,
        )

    def onward(a, j):
        half = pl.ds((j - 1) * (TOKENS_HERE // 2), TOKENS_HERE // 2)
        part = pl.ds(0, COLUMNS[a][1])
        return pltpu.make_async_remote_copy(
            ring_rows.at[a, j, half, part], ring_rows.at[a, 3, half, part],
            far_send.at[a, j], far_recv.at[a, j],
            device_id=here.along(a, OFFSETS[j]), device_id_type=MESH,
        )

    for j in (1, 2):
        for a in range(ORDERS):
            ring(a, j).start()

    def block(ref, index, a):
        first, width = COLUMNS[a]
        return ref.at[(*index, pl.ds(0, CAP), pl.ds(first, width))]

    def ship(dc, lead):
        for u in range(SIDE):
            for v in range(SIDE):
                if u or v or dc:
                    for a in range(ORDERS):
                        spot = [(u, v, 0), (u, 0, v), (0, u, v)][a]
                        index = [(u, v, lead), (u, lead, v), (lead, u, v)][a]
                        sem = box_id(a, dc, 0 if u else 1)
                        pltpu.make_async_remote_copy(
                            block(outgoing, (*index, dc), a), block(arrived, (*index, dc), a),
                            out_send.at[sem], out_recv.at[sem],
                            device_id=here.spot(*spot, dc, 1), device_id_type=MESH,
                        ).start()

    def plane(a, j):
        first, width = COLUMNS[a]
        every, columns = slice(None), slice(first, first + width)
        lead = [(every, every, j), (every, j, every), (j, every, every)][a]
        return (*lead, every, every, columns)

    def local(a):
        first, width = COLUMNS[a]
        every, columns = slice(None), slice(first, first + width)
        lead = [(0, 0, every, 0), (0, every, 0, 0), (every, 0, 0, 0)][a]
        return (*lead, every, columns)

    def fill(a, j, rows):
        value = dot(place[a * SIDE + j], rows).astype(BF16)
        outgoing[plane(a, j)] = value.reshape(SIDE, SIDE, 2, SLOTS, COLUMNS[a][1])

    for a, (first, width) in enumerate(COLUMNS):
        fill(a, 0, normed[:, first : first + width])
    pl.semaphore_wait(cube_sem, SIDE - 1)
    for dc in WAVES:
        ship(dc, 0)

    others = pl.ds(1, SIDE - 1)
    pltpu.make_async_remote_copy(
        ring_ids.at[:, others], ring_ids.at[:, others], table_send, table_recv,
        device_id=(sp, 1 - tp), device_id_type=MESH,
    ).wait()
    for a in range(ORDERS):
        for j in (1, 2):
            set_place(a, j, tag_of(ring_ids[a, j]))
    for j in (1, 2):
        for a in range(ORDERS):
            ring(a, j).wait_recv()
            onward(a, j).start()
    for j in (1, 2):
        for a in range(ORDERS):
            fill(a, j, ring_rows[a, j, :, : COLUMNS[a][1]])
    ship(WAVES[0], pl.ds(1, 2))
    for a in range(ORDERS):
        set_place(a, 3, tag_of(ring_ids[a, 3]))
    for a in range(ORDERS):
        onward(a, 1).wait_recv()
        onward(a, 2).wait_recv()
        fill(a, 3, ring_rows[a, 3, :, : COLUMNS[a][1]])
    ship(WAVES[0], 3)
    ship(WAVES[1], pl.ds(1, 2))
    ship(WAVES[1], 3)
    for a in range(ORDERS):
        arrived[local(a)] = outgoing[local(a)]

    def clear(i, _):
        returned[i // SIDE, i % SIDE, :, :, CAP:, :] = jnp.zeros((SIDE, 2, SLOTS - CAP, D), BF16)
        return 0

    lax.fori_loop(0, SIDE * SIDE, clear, 0)

    get_eg.wait()
    get_eu.wait()
    get_ed.wait()

    def beside():
        get_sg.wait()
        get_su.wait()
        get_sd.wait()
        hidden = dot(normed[...], sg[...])
        hidden = hidden / (1.0 + jnp.exp(-hidden)) * dot(normed[...], su[...])
        hidden = hidden.astype(BF16)
        for n in range(0, D, 512):
            acc[:, n : n + 512] = settled[:, n : n + 512].astype(F32) + dot(hidden, sd[:, n : n + 512])


        raw = score[...]
        weights = raw / jnp.sum(raw, axis=0, keepdims=True) * routed_scale
        weight = jnp.zeros((DEVICES, TOKENS_HERE), F32)
        for k in range(TOPK):
            weight = jnp.where(expert == ids[k : k + 1, :], weights[k : k + 1, :], weight)
        high = weight.astype(BF16)
        low = (weight - high.astype(F32)).astype(BF16)
        w, u, v = slot_row // 64, slot_row // 16 % SIDE, slot_row // 8 % 2
        w, u = [jnp.where(i < 2, i, 5 - i) for i in (w, u)]
        for dc in range(2):
            for half in range(2):
                along = 3 - v if half else v
                chip = ((z + w) % SIDE * SIDE + (y + u) % SIDE) * SIDE + (x + along) % SIDE
                over = (chip * 2 + (tp + dc) % 2 == slot_expert).astype(BF16)
                where = (dot(over, own_tag) == slot_number).astype(F32)
                comb[2 * dc + half, :TOKENS_HERE, :] = (dot(over, high) * where).T.astype(BF16)
                comb[2 * dc + half, TOKENS_HERE:, :] = (dot(over, low) * where).T.astype(BF16)

    def box(a, dc, i):
        index, sem = boxes(a, dc)[i], box_id(a, dc, i)
        return pltpu.make_async_remote_copy(
            block(outgoing, index, a), block(arrived, index, a), out_send.at[sem], out_recv.at[sem],
            device_id=(sp, 1 - tp), device_id_type=MESH,
        )

    def back_copy(index, sem, device):
        index = (*index, pl.ds(0, CAP))
        return pltpu.make_async_remote_copy(
            results.at[index], returned.at[index], back_send.at[sem], back_recv.at[sem],
            device_id=device, device_id_type=MESH,
        )

    def back_box(dc, half, i):
        index = back_boxes(dc, half)[i]
        return back_copy(index, back_id(dc, half, i), (sp, 1 - tp))

    for dc in WAVES:
        for a in range(ORDERS):
            for i in range(len(boxes(a, dc))):
                box(a, dc, i).wait_recv()
        for half in HALVES:
            xs = slice(2 * half, 2 * half + 2)
            rows = arrived[:, :, xs, dc].reshape(RINGS, D)
            hidden = dot(rows, eg[...])
            hidden = hidden / (1.0 + jnp.exp(-hidden)) * dot(rows, eu[...])
            hidden = hidden.astype(BF16)
            for n in range(0, D, 512):
                value = dot(hidden, ed[:, n : n + 512]).astype(BF16)
                results[:, :, xs, dc, :, n : n + 512] = value.reshape(SIDE, SIDE, 2, SLOTS, 512)
            for spot, i in back_spots(dc, half):
                back_copy((*spot, dc), back_id(dc, half, i), here.spot(*spot, dc, -1)).start()
        if dc == WAVES[0]:
            beside()
    returned[0, 0, 0, 0] = results[0, 0, 0, 0]

    for dc in WAVES:
        for half in HALVES:
            for i in range(len(back_boxes(dc, half))):
                back_box(dc, half, i).wait_recv()
            for n in range(0, D, 512):
                rows = returned[:, :, 2 * half : 2 * half + 2, dc, :, n : n + 512]
                both = dot(comb[2 * dc + half], rows.reshape(RINGS, 512))
                value = acc[:, n : n + 512] + (both[:TOKENS_HERE] + both[TOKENS_HERE:])
                if dc != WAVES[-1] or half != HALVES[-1]:
                    acc[:, n : n + 512] = value
                else:
                    out_ref[:, n : n + 512] = value.astype(BF16)

    for dc in range(2):
        for a in range(ORDERS):
            for i in range(len(boxes(a, dc))):
                box(a, dc, i).wait_send()
        for half in range(2):
            for i in range(len(back_boxes(dc, half))):
                back_box(dc, half, i).wait_send()
    for a in range(ORDERS):
        for j in (1, 2):
            ring(a, j).wait_send()
            onward(a, j).wait_send()


def on_device(
    residual, pool_input, group_maps, pool_scale, out_proj, norm_gain,
    shared_gate, shared_up, shared_down, expert_gate, expert_up, expert_down,
    expert_ids, route_score,
):
    any_space = pl.BlockSpec(memory_space=pl.ANY)
    vmem = pltpu.VMEM
    block = (SIDE, SIDE, SIDE, 2, SLOTS, D)
    dma = pltpu.SemaphoreType.DMA
    return pl.pallas_call(
        kernel,
        name="mixer_experts",
        out_shape=pltpu.VMEM((TOKENS_HERE, D), BF16),
        in_specs=[any_space] * 14,
        out_specs=pl.BlockSpec(memory_space=pltpu.VMEM),
        scratch_shapes=[
            vmem((TOKENS_HERE, D), BF16),
            vmem((REACH + ROWS, CHANNELS), BF16),
            vmem((2 * GROUPS, GW, GW), BF16),
            vmem((8, 128), F32),
            vmem((2 * CHANNELS, D), BF16),
            vmem((D // 128, 128), F32),
            vmem((D, HID), BF16),
            vmem((D, HID), BF16),
            vmem((HID, D), BF16),
            vmem((D, HID), BF16),
            vmem((D, HID), BF16),
            vmem((HID, D), BF16),
            vmem((TOPK, TOKENS_HERE), jnp.int32),
            vmem((TOPK, TOKENS_HERE), F32),
            vmem((TOKENS_HERE, CHANNELS), BF16),
            vmem((REACH + TOKENS_HERE, CHANNELS), BF16),
            vmem((2, REACH, CHANNELS), BF16),
            vmem((TOKENS_HERE, D), BF16),
            vmem((TOKENS_HERE, D), BF16),
            vmem((TOKENS_HERE, D), F32),
            vmem((ORDERS, SIDE, TOPK, TOKENS_HERE), jnp.int32),
            vmem((ORDERS * SIDE, RINGS, TOKENS_HERE), BF16),
            vmem((4, 2 * TOKENS_HERE, RINGS), BF16),
            vmem((ORDERS, SIDE, TOKENS_HERE, WIDEST), BF16),
            vmem(block, BF16),
            vmem(block, BF16),
            vmem(block, BF16),
            vmem(block, BF16),
            dma((14,)),
            dma((2,)), dma((2,)), dma, dma,
            dma, dma, dma((ORDERS, SIDE)), dma((ORDERS, SIDE)), dma((ORDERS, SIDE)), dma((ORDERS, SIDE)),
            dma((9,)), dma((9,)), dma((6,)), dma((6,)),
            pltpu.SemaphoreType.REGULAR,
            pltpu.SemaphoreType.REGULAR,
        ],
        compiler_params=pltpu.CompilerParams(
            collective_id=0, has_side_effects=True, vmem_limit_bytes=60 << 20
        ),
    )(
        residual, pool_input, group_maps, pool_scale.reshape(8, 128), out_proj,
        norm_gain.reshape(D // 128, 128), shared_gate, shared_up, shared_down,
        expert_gate, expert_up, expert_down, expert_ids.T, route_score.T,
    )


def solution(mesh):
    in_specs = (
        P(("sp", "tp"), None),
        P("sp", "tp"),
        P(), P(), P(), P(), P(), P(), P(),
        P(("sp", "tp"), None, None),
        P(("sp", "tp"), None, None),
        P(("sp", "tp"), None, None),
        P(("sp", "tp"), None),
        P(("sp", "tp"), None),
    )
    return jax.shard_map(
        on_device, mesh=mesh, in_specs=in_specs, out_specs=P(("sp", "tp"), None), check_vma=False
    )
```
